256 devices in a mesh: ep: 128 (over z, y, x), tp: 2 (over core).
Axes of the slice: x: 4, y: 4, z: 8, core: 2. Of those that a mesh axis runs over, the one named last changes fastest.
Arguments:
- tokens: bfloat16 [4096, 1024], P('ep'), may hold values from -6 to 6
- norm_gain: float32 [1024], replicated, may hold values from 0.1 to 1.9
- routing: int32 [4096, 4], P('ep'), may hold values from 0 to 127, all different within a row; in each aligned block of 32 rows (0 to 31, 32 to 63, ...) at most 16 rows name the same one
- route_logits: float32 [4096, 4], P('ep'), may hold values from -6 to 6
- w_gate: bfloat16 [128, 1024, 1024], P('ep', None, 'tp'), may hold values from -0.1875 to 0.1875
- w_up: bfloat16 [128, 1024, 1024], P('ep', None, 'tp'), may hold values from -0.1875 to 0.1875
- w_down: bfloat16 [128, 1024, 1024], P('ep', None, 'tp'), may hold values from -0.1875 to 0.1875
Outputs:
- mixed: bfloat16 [4096, 1024], P('ep', 'tp')
The draws below stay inside these ranges and needn't reach their ends.
Inputs may be any that keep to these rules, and one draw needn't show every extreme that they name: `routing`: each row names 4 different experts; among the 32 tokens of one index of ep (aligned blocks of rows) no expert is named by more than 16 rows, and some block has an expert named by exactly 16.
All inputs are finite; a program needn't handle non-finite values.
Results may differ from the reference program's by a relative error of at most 0.0085.
Values may be sent and summed in bfloat16 or wider, within the bound.
A program may use at most 64 MiB of HBM per device.

```python
import math
import jax
import jax.numpy as jnp
import numpy as np
from jax import lax

D = 1024
FF = 1024
TOPK = 4
TOK_DEV = 32
TOKENS = 4096
EXPERTS = 128
CAP = 16


def block_levels(stream_key, dims, shards, smallest, largest):
    def one(axis_at, parts):
        steps = jax.random.uniform(jax.random.fold_in(jax.random.fold_in(stream_key, 6), axis_at), (parts,), jnp.float32, smallest / len(shards), largest / len(shards))
        return jnp.repeat(jnp.exp(steps), dims[axis_at] // parts).reshape((-1,) + (1,) * (len(dims) - axis_at - 1))

    level = one(*shards[0])
    for cut in shards[1:]:
        level = level * one(*cut)
    return level


def routed_block(stream_key, own, number, rows, count, top, reach, skew):
    ranking = jax.random.permutation(stream_key, count)
    packed, ordinary = portions_of(count, rows * top, reach, skew, True), portions_of(count, rows * top, reach, skew, False)
    places = jnp.arange(count)

    def named(tallies, rotation):
        used = int((tallies > 0).sum())
        fixed = max(1, used // 4)
        passed = fixed + (places - fixed + rotation * (used - fixed)) % max(1, count - fixed)
        return jnp.zeros((count,), jnp.int32).at[ranking[jnp.where(places < fixed, places, passed)]].set(jnp.asarray(tallies, jnp.int32))

    tallies = jnp.where(number % 4 == 0, named(packed, number // 4), named(ordinary, number - number // 4 - 1))
    mixed = jax.random.permutation(jax.random.fold_in(own, 3), count)
    donor, taker = mixed[0:count // 2 * 2:2], mixed[1:count // 2 * 2:2]
    slack = jnp.minimum(tallies[donor] - 1, reach - tallies[taker]) // 2
    slack = jnp.where((donor == ranking[0]) | (taker == ranking[0]) | (tallies[taker] == 0), 0, jnp.maximum(slack, 0))
    passed = jax.random.randint(jax.random.fold_in(own, 4), (count // 2,), 0, 1 << 20) % (slack + 1)
    tallies = tallies.at[donor].add(-passed).at[taker].add(passed)
    members = jnp.searchsorted(jnp.cumsum(tallies), jnp.arange(rows * top), side="right").astype(jnp.int32)
    listing = members.reshape(top, rows).T
    listing = listing[jax.random.permutation(jax.random.fold_in(own, 1), rows)]
    rotation = jax.random.randint(jax.random.fold_in(own, 2), (rows, 1), 0, top)
    return jnp.take_along_axis(listing, (jnp.arange(top)[None, :] + rotation) % top, axis=1)


def portions_of(amount, total, bound, lean, full):
    portions = [(1 << 20) // math.isqrt(rank ** lean) + 1 for rank in range(1, amount + 1)]
    largest = bound if full else min(bound, max(-(-total // amount), total * portions[0] // sum(portions)))
    least = 1 if total - largest >= amount - 1 else 0
    given, surplus = [largest] + [least] * (amount - 1), total - largest - least * (amount - 1)
    while surplus > 0:
        candidates = [i for i in range(1, amount) if given[i] < largest] or [i for i in range(1, amount) if given[i] < bound]
        pool, remaining = sum([portions[i] for i in candidates]), surplus
        for i in candidates:
            more = min(bound - given[i], max(1, remaining * portions[i] // pool), surplus)
            given[i] = given[i] + more
            surplus = surplus - more
    return np.array(given)


def bell_draw(key, shape, spread, most, split=(), held_as=jnp.bfloat16):
    array = jax.random.normal(key, shape, jnp.float32) * spread
    if len(split) > 0:
        array = block_levels(key, shape, split, -0.22, 0.18) * array
    return jnp.clip(array, min=-most, max=most).astype(held_as)


def setup_inputs(seed: int = 0) -> dict:
    key_list = jax.random.split(jax.random.key(seed), 8)
    tokens = bell_draw(key_list[0], (TOKENS, D), 1.0, 6.0, ((0, 128),))
    norm_gain = jnp.clip(1.0 + 0.18 * jax.random.normal(key_list[1], (D,), jnp.float32), 0.1, 1.9)
    routing_keys = jax.random.split(jax.random.fold_in(key_list[2], 1), TOKENS // TOK_DEV)
    routing_turns = jax.random.permutation(jax.random.fold_in(key_list[2], 3), TOKENS // TOK_DEV)
    routing = jax.vmap(lambda own, number: routed_block(jax.random.fold_in(key_list[2], 2), own, number, TOK_DEV, EXPERTS, TOPK, CAP, 2))(routing_keys, routing_turns).reshape((TOKENS, TOPK))
    route_logits = bell_draw(key_list[3], (TOKENS, TOPK), 1.5, 6.0, ((0, 128),), jnp.float32)
    w_gate = bell_draw(key_list[4], (EXPERTS, D, FF), D ** -0.5, 0.1875, ((0, 128), (2, 2)))
    w_up = bell_draw(key_list[5], (EXPERTS, D, FF), D ** -0.5, 0.1875, ((0, 128), (2, 2)))
    w_down = bell_draw(key_list[6], (EXPERTS, FF, D), FF ** -0.5, 0.1875, ((0, 128), (2, 2)))
    return dict(tokens=tokens, norm_gain=norm_gain, routing=routing, route_logits=route_logits, w_gate=w_gate, w_up=w_up, w_down=w_down)


eps = 1e-5


def clamped(gate_part, up_part):
    limited = jnp.minimum(gate_part, 7.0)
    linear = jnp.clip(up_part, -7.0, 7.0)
    return limited * jax.nn.sigmoid(1.702 * limited) * (linear + 1.0)


def reference(tokens, norm_gain, routing, route_logits, w_gate, w_up, w_down):
    as_float = tokens.astype(jnp.float32)
    scaled = as_float * lax.rsqrt(jnp.mean(as_float * as_float, axis=-1, keepdims=True) + eps)
    normed = (scaled * norm_gain).astype(jnp.bfloat16)
    probs = jax.nn.softmax(route_logits, axis=-1)
    count_tok = routing.shape[0]
    topk = routing.shape[1]
    assigns = count_tok * topk
    block_rows = 32
    flat_e = routing.reshape(-1).astype(jnp.int32)
    flat_tok = (jnp.arange(assigns, dtype=jnp.int32) // topk).astype(jnp.int32)
    flat_w = probs.reshape(-1)
    order = jnp.argsort(flat_e, stable=True).astype(jnp.int32)
    sorted_e = flat_e[order]
    counts = jnp.bincount(flat_e, length=EXPERTS).astype(jnp.int32)
    starts = (jnp.cumsum(counts) - counts).astype(jnp.int32)
    padded = ((counts + block_rows - 1) // block_rows * block_rows).astype(jnp.int32)
    pends = jnp.cumsum(padded).astype(jnp.int32)
    pstarts = (pends - padded).astype(jnp.int32)
    dest = (pstarts[sorted_e] + jnp.arange(assigns, dtype=jnp.int32) - starts[sorted_e]).astype(jnp.int32)
    n_blocks = -(-assigns // block_rows) + EXPERTS
    n_rows = n_blocks * block_rows
    row_tok = jnp.full((n_rows,), count_tok, dtype=jnp.int32).at[dest].set(flat_tok[order])
    row_w = jnp.zeros((n_rows,), jnp.float32).at[dest].set(flat_w[order])
    block_e = jnp.minimum(
        jnp.searchsorted(pends, jnp.arange(n_blocks, dtype=jnp.int32) * block_rows, side="right").astype(jnp.int32),
        EXPERTS - 1).astype(jnp.int32)
    x_pad = jnp.concatenate([normed, jnp.zeros((1, normed.shape[1]), jnp.bfloat16)], axis=0)
    blocks_in = x_pad[row_tok].reshape(n_blocks, block_rows, normed.shape[1])

    def expert_block(pair):
        rows, expert = pair
        gate_part = jnp.dot(rows, w_gate[expert], preferred_element_type=jnp.float32)
        up_part = jnp.dot(rows, w_up[expert], preferred_element_type=jnp.float32)
        hidden = clamped(gate_part, up_part).astype(jnp.bfloat16)
        return jnp.dot(hidden, w_down[expert], preferred_element_type=jnp.float32).astype(jnp.bfloat16)

    outs_rows = lax.map(expert_block, (blocks_in, block_e)).reshape(n_rows, normed.shape[1])
    summed = jax.ops.segment_sum(outs_rows.astype(jnp.float32) * row_w[:, None], row_tok, num_segments=count_tok + 1)
    return summed[:count_tok].astype(jnp.bfloat16)
```

```python
import jax
import jax.numpy as jnp
from jax import lax
from jax.sharding import PartitionSpec as P

eps = 1e-05


def clamped(gate_part, up_part):
    limited = jnp.minimum(gate_part, 7.0)
    linear = jnp.clip(up_part, -7.0, 7.0)
    return limited * jax.nn.sigmoid(1.702 * limited) * (linear + 1.0)


def shards(tokens, norm_gain, routing, route_logits, w_gate, w_up, w_down):
    as_float = tokens.astype(jnp.float32)
    scaled = as_float * lax.rsqrt(jnp.mean(as_float * as_float, axis=-1, keepdims=True) + eps)
    normed = (scaled * norm_gain).astype(jnp.bfloat16)
    probs = jax.nn.softmax(route_logits, axis=-1)
    half = normed.shape[1] // 2
    mine = lax.dynamic_slice_in_dim(normed, lax.axis_index("tp") * half, half, 1)
    n_ep = lax.axis_size("ep")
    expert = lax.axis_index("ep")
    onehot = routing[:, :, None] == jnp.arange(n_ep, dtype=jnp.int32)
    weights = jnp.sum(jnp.where(onehot, probs[:, :, None], 0.0), axis=1)
    arrived_w = lax.all_to_all(weights.T, "ep", split_axis=0, concat_axis=0, tiled=True)
    rows = lax.all_gather(mine, "ep", axis=0, tiled=True)
    rows = lax.all_gather(rows, "tp", axis=1, tiled=True)
    gate_part = jnp.dot(rows, w_gate[0], preferred_element_type=jnp.float32)
    up_part = jnp.dot(rows, w_up[0], preferred_element_type=jnp.float32)
    hidden = clamped(gate_part, up_part).astype(jnp.bfloat16)
    hidden = lax.all_gather(hidden, "tp", axis=1, tiled=True)
    out = jnp.dot(hidden, w_down[0], preferred_element_type=jnp.float32)
    out = out * arrived_w.reshape(-1, 1)
    return lax.psum_scatter(out.astype(jnp.bfloat16), "ep", scatter_dimension=0, tiled=True)


def solution(mesh):
    return jax.shard_map(
        shards,
        mesh=mesh,
        in_specs=(
            P("ep", None),
            P(),
            P("ep", None),
            P("ep", None),
            P("ep", None, "tp"),
            P("ep", None, "tp"),
            P("ep", None, "tp"),
        ),
        out_specs=P("ep", "tp"),
        check_vma=False,
    )
```

```python
import jax
import jax.numpy as jnp
from jax import lax
from jax.experimental import pallas as pl
from jax.experimental.pallas import tpu as pltpu
from jax.sharding import PartitionSpec as P

MESH = pl.DeviceIdType.MESH
NX, NY, NZ = 4, 4, 8
CAP = 16
BLK = 32
HALF = 256
ROWS = BLK + 8
EPS = 1e-05
BF = jnp.bfloat16
F32 = jnp.float32
ARRIVAL = (0, 1, 7, 2, 6, 3, 5, 4)


def iota(shape, dim):
    return lax.broadcasted_iota(jnp.int32, shape, dim)


def kernel(
    tok_hbm, gain_hbm, ids_hbm, log_hbm, wg_hbm, wu_hbm, wd_hbm, out_ref,
    tok, gain, ids, logits, wg, wu, wd,
    own, ybuf, sbuf, xown, xoth, hown, hoth, ysend, r1buf, pacc, r2send, r2buf, r3send, r3buf,
    in_sem, w_sem, z_send, z_recv, s2_send, s2_recv, s3_send, s3_recv, x_send, x_recv,
    h_send, h_recv, r1_send, r1_recv, r2_send, r2_recv, r3_send, r3_recv,
):
    ep = lax.axis_index("ep")
    c = lax.axis_index("tp")
    x = lax.rem(ep, NX)
    y = lax.rem(ep // NX, NY)
    z = ep // (NX * NY)

    def at(dx=0, dy=0, dz=0):
        px = lax.rem(x + dx, NX)
        py = lax.rem(y + dy, NY)
        pz = lax.rem(z + dz, NZ)
        return ((pz * NY + py) * NX + px, c)

    partner = (ep, 1 - c)

    def peer(col, j):
        return at(dy=j) if col == 0 else at(dx=j)

    def far(col, j):
        return at(dx=j) if col == 0 else at(dy=j)

    def remote(src, dst, send, recv, device):
        return pltpu.make_async_remote_copy(
            src_ref=src, dst_ref=dst, send_sem=send, recv_sem=recv, device_id=device, device_id_type=MESH
        )

    def drain(ref, sem):
        pltpu.make_async_copy(ref, ref, sem).wait()

    small = [
        pltpu.make_async_copy(tok_hbm, tok, in_sem.at[0]),
        pltpu.make_async_copy(gain_hbm, gain, in_sem.at[1]),
        pltpu.make_async_copy(ids_hbm, ids, in_sem.at[2]),
        pltpu.make_async_copy(log_hbm, logits, in_sem.at[3]),
    ]
    for copy in small:
        copy.start()
    weights = []
    for i, (src, dst) in enumerate(((wg_hbm, wg), (wu_hbm, wu), (wd_hbm, wd))):
        for part in range(2):
            start = pl.multiple_of(lax.rem(c + part, 2) * 512, 512)
            weights.append(
                pltpu.make_async_copy(src.at[pl.ds(start, 512)], dst.at[pl.ds(part * 512, 512)], w_sem.at[i, part])
            )
    for copy in weights:
        copy.start()

    barrier = pltpu.get_barrier_semaphore()
    friends = [at(dz=k) for k in range(1, NZ)] + [at(dy=j) for j in range(1, NY)] + [at(dx=j) for j in range(1, NX)]
    friends.append(partner)
    for friend in friends:
        pl.semaphore_signal(barrier, inc=1, device_id=friend, device_id_type=MESH)

    for copy in small:
        copy.wait()

    full = tok[...].astype(F32)
    scale = lax.rsqrt(jnp.mean(full * full, axis=-1, keepdims=True) + EPS)
    mine = pl.ds(pl.multiple_of(c * 512, 512), 512)
    normed = (tok[:, mine].astype(F32) * scale * gain[:, mine]).astype(BF)

    lane4 = iota((BLK, 128), 1)
    spread = (lax.rem(lane4, BLK) == iota((BLK, 128), 0)).astype(BF)
    raw = logits[...]
    shifted = jnp.exp(raw - jnp.max(raw, axis=0, keepdims=True))
    probs = shifted / jnp.sum(shifted, axis=0, keepdims=True)
    ids_l = jnp.dot(ids[...].astype(F32).astype(BF), spread, preferred_element_type=F32)
    probs_l = jnp.dot(probs.astype(BF), spread, preferred_element_type=F32)
    row = iota((128, 128), 0)
    lane = iota((128, 128), 1)
    plane = lax.rem(z + row // 16, NZ)
    near = lax.rem(row, 4)
    group = lane // BLK
    route_b = lax.rem(row // 8, 2) == 0
    ex = lax.rem(x + jnp.where(route_b, near, group), NX)
    ey = lax.rem(y + jnp.where(route_b, group, near), NY)
    expert = (plane * 16 + ey * NX + ex).astype(F32)
    named = jnp.zeros((128, 128), F32)
    weight = jnp.zeros((128, 128), F32)
    for q in range(4):
        hit = expert == ids_l[q : q + 1, :]
        named = jnp.where(hit, 1.0, named)
        weight = jnp.where(hit, probs_l[q : q + 1, :], weight)
    before = ((row // BLK == lane // BLK) & (row < lane)).astype(BF)
    place = jnp.dot(named.astype(BF), before, preferred_element_type=F32)
    place = jnp.where(named > 0, place, -128.0)
    meta = jnp.where(lax.rem(row, 8) < 4, place, weight).astype(BF)
    blank = jnp.zeros((8, HALF - 128), BF)
    for k in range(NZ):
        for col in range(2):
            dst = own.at[k, col] if k else ybuf.at[0, col, 0]
            dst[:BLK, :] = normed[:, col * HALF : (col + 1) * HALF]
            dst[BLK:, :128] = meta[k * 16 + col * 8 : k * 16 + col * 8 + 8, :]
            dst[BLK:, 128:] = blank

    pl.semaphore_wait(barrier, len(friends))

    def start_z():
        for k in (1, 7, 2, 6, 3, 5, 4):
            slot = (-k) % NZ
            remote(own.at[k], ybuf.at[slot, :, 0], z_send, z_recv.at[slot], at(dz=k)).start()

    def s2(k):
        if k:
            drain(own.at[k], z_recv.at[k])
        for j in (1, 3, 2):
            for col in range(2):
                remote(
                    ybuf.at[k, col, 0], ybuf.at[k, col, (-j) % 4], s2_send, s2_recv.at[k, col], peer(col, j)
                ).start()

    lanes = iota((8, 128), 1) // BLK
    sixty = iota((64, 128), 0)
    base = (iota((1, 128), 1) // BLK * CAP).astype(F32)

    def table(k, col):
        t = [ybuf[k, col, s, BLK:, :128].astype(F32) for s in range(4)]
        t1 = pltpu.roll(t[1], 64, 1)
        t3 = pltpu.roll(t[3], 64, 1)
        return jnp.where(lanes == 0, t[0], jnp.where(lanes == 1, t1, jnp.where(lanes == 2, t[2], t3)))

    def select(k, col, weighted):
        m = table(k, col)
        parts = []
        for j in range(4):
            wanted = (m[j : j + 1, :] + base).astype(jnp.int32)
            value = m[4 + j : 5 + j, :] if weighted else 1.0
            parts.append(jnp.where(sixty == wanted, value, 0.0).astype(BF))
        return jnp.concatenate(parts, axis=0)

    def s3(k):
        for col in range(2):
            drain(ybuf.at[k, col, pl.ds(1, 3)], s2_recv.at[k, col])
            rows = ybuf[k, col, :, :BLK, :].reshape(128, HALF)
            packed = jnp.dot(select(k, col, False), rows, preferred_element_type=F32).astype(BF)
            for j in range(4):
                piece = packed[64 * j : 64 * j + 64].reshape(4, CAP, HALF)
                if j:
                    sbuf[k, col, j - 1] = piece
                elif col == 0:
                    xown[k, 0, 0] = piece
                else:
                    xown[k, 1, :, 0] = piece
            for j in (1, 3, 2):
                slot = (-j) % 4
                dst = xown.at[k, 0, slot] if col == 0 else xown.at[k, 1, :, slot]
                remote(sbuf.at[k, col, j - 1], dst, s3_send, s3_recv.at[k, col], far(col, j)).start()

    def x4(k):
        for col in range(2):
            drain(sbuf.at[k, col], s3_recv.at[k, col])
        remote(xown.at[k], xoth.at[k], x_send, x_recv.at[k], partner).start()

    def g5(k):
        drain(xoth.at[k], x_recv.at[k])
        rows = jnp.concatenate([ref[k, col].reshape(256, HALF) for ref in (xown, xoth) for col in range(2)], axis=1)
        gate = jnp.minimum(jnp.dot(rows, wg[...], preferred_element_type=F32), 7.0)
        lin = jnp.clip(jnp.dot(rows, wu[...], preferred_element_type=F32), -7.0, 7.0)
        sig = 0.5 * jnp.tanh(0.851 * gate) + 0.5
        hown[k] = (gate * sig * (lin + 1.0)).astype(BF)
        remote(hown.at[k], hoth.at[k], h_send, h_recv.at[k], partner).start()

    def d6(k):
        drain(hoth.at[k], h_recv.at[k])
        hidden = jnp.concatenate([hown[k], hoth[k]], axis=1)
        done = jnp.dot(hidden, wd[...], preferred_element_type=F32).astype(BF)
        for col in range(2):
            rows = done[:, col * HALF : (col + 1) * HALF].reshape(4, 4, CAP, HALF)
            for j in range(4):
                piece = rows[j] if col == 0 else rows[:, j]
                if j:
                    ysend[k, col, j - 1] = piece
                else:
                    r1buf[k, col, 0] = piece
            for j in (1, 3, 2):
                remote(
                    ysend.at[k, col, j - 1], r1buf.at[k, col, (-j) % 4], r1_send, r1_recv.at[k, col], far(col, j)
                ).start()

    def u7(k):
        for col in range(2):
            drain(ysend.at[k, col], r1_recv.at[k, col])
            rows = r1buf[k, col].reshape(256, HALF)
            sums = lax.dot_general(
                select(k, col, True), rows, (((0,), (0,)), ((), ())), preferred_element_type=F32
            )
            pacc[k, col] = sums[:BLK]
            for j in range(1, 4):
                r2send[k, col, j - 1] = sums[BLK * j : BLK * j + BLK].astype(BF)
            for j in (1, 3, 2):
                remote(
                    r2send.at[k, col, j - 1], r2buf.at[k, col, (-j) % 4 - 1], r2_send, r2_recv.at[k, col], peer(col, j)
                ).start()

    def r8(k):
        for col in range(2):
            drain(r2buf.at[k, col], r2_recv.at[k, col])
            total = pacc[k, col]
            for j in range(3):
                total = total + r2buf[k, col, j].astype(F32)
            if k:
                r3send[k, col] = total.astype(BF)
            else:
                pacc[0, col] = total
        if k:
            slot = (-k) % NZ
            remote(r3send.at[k], r3buf.at[slot], r3_send, r3_recv.at[slot], at(dz=k)).start()

    start_z()
    n = NZ
    order = ARRIVAL
    back = order[1:] + order[:1]
    s2(order[0])
    ready = False
    for i in range(n + 7):
        if i + 1 < n:
            s2(order[i + 1])
        if i < n:
            s3(order[i])
        if 0 <= i - 1 < n:
            x4(order[i - 1])
        if 0 <= i - 2 < n:
            if not ready:
                for copy in weights:
                    copy.wait()
                ready = True
            g5(order[i - 2])
        if 0 <= i - 3 < n:
            d6(order[i - 3])
        if 0 <= i - 5 < n:
            u7(order[i - 5])
        if 0 <= i - 6 < n:
            r8(order[i - 6])

    for col in range(2):
        total = pacc[0, col]
        for k in range(1, NZ):
            if col == 0:
                drain(r3buf.at[k], r3_recv.at[k])
            total = total + r3buf[k, col].astype(F32)
        out_ref[:, col * HALF : (col + 1) * HALF] = total.astype(BF)

    drain(own.at[pl.ds(1, 7)], z_send)
    drain(ybuf.at[:, :, pl.ds(1, 3)], s2_send)
    drain(sbuf, s3_send)
    drain(xown, x_send)
    drain(hown, h_send)
    drain(ysend, r1_send)
    drain(r2send, r2_send)
    drain(r3send.at[pl.ds(1, 7)], r3_send)


def shards(tokens, norm_gain, routing, route_logits, w_gate, w_up, w_down):
    vmem = pltpu.VMEM
    dma = pltpu.SemaphoreType.DMA
    return pl.pallas_call(
        kernel,
        name="routed_layer",
        out_shape=jax.ShapeDtypeStruct((BLK, 2 * HALF), BF),
        in_specs=[pl.BlockSpec(memory_space=pl.ANY)] * 7,
        out_specs=pl.BlockSpec(memory_space=vmem),
        scratch_shapes=[
            vmem((BLK, 1024), BF),
            vmem((1, 1024), F32),
            vmem((4, BLK), jnp.int32),
            vmem((4, BLK), F32),
            vmem((1024, 512), BF),
            vmem((1024, 512), BF),
            vmem((1024, 512), BF),
            vmem((NZ, 2, ROWS, HALF), BF),
            vmem((NZ, 2, 4, ROWS, HALF), BF),
            vmem((NZ, 2, 3, 4, CAP, HALF), BF),
            vmem((NZ, 2, 4, 4, CAP, HALF), BF),
            vmem((NZ, 2, 4, 4, CAP, HALF), BF),
            vmem((NZ, 256, 512), BF),
            vmem((NZ, 256, 512), BF),
            vmem((NZ, 2, 3, 4, CAP, HALF), BF),
            vmem((NZ, 2, 4, 4, CAP, HALF), BF),
            vmem((NZ, 2, BLK, HALF), F32),
            vmem((NZ, 2, 3, BLK, HALF), BF),
            vmem((NZ, 2, 3, BLK, HALF), BF),
            vmem((NZ, 2, BLK, HALF), BF),
            vmem((NZ, 2, BLK, HALF), BF),
            dma((4,)),
            dma((3, 2)),
            dma, dma((NZ,)),
            dma, dma((NZ, 2)),
            dma, dma((NZ, 2)),
            dma, dma((NZ,)),
            dma, dma((NZ,)),
            dma, dma((NZ, 2)),
            dma, dma((NZ, 2)),
            dma, dma((NZ,)),
        ],
        compiler_params=pltpu.CompilerParams(
            collective_id=0, has_side_effects=True, vmem_limit_bytes=60 * 1024 * 1024
        ),
    )(tokens, norm_gain.reshape(1, -1), routing.T, route_logits.T, w_gate[0], w_up[0], w_down[0])


def solution(mesh):
    return jax.shard_map(
        shards,
        mesh=mesh,
        in_specs=(
            P("ep", None),
            P(),
            P("ep", None),
            P("ep", None),
            P("ep", None, "tp"),
            P("ep", None, "tp"),
            P("ep", None, "tp"),
        ),
        out_specs=P("ep", "tp"),
        check_vma=False,
    )
```

```python
import jax
import jax.numpy as jnp
from jax import lax
from jax.experimental import pallas as pl
from jax.experimental.pallas import tpu as pltpu
from jax.sharding import PartitionSpec as P

MESH = pl.DeviceIdType.MESH
NX, NY, NZ = 4, 4, 8
CAP = 16
BLK = 32
HALF = 256
ROWS = BLK + 8
EPS = 1e-05
BF = jnp.bfloat16
F32 = jnp.float32
SEQ = (
    (0, 0, 1), (0, 0, 0), (0, 7, 1), (0, 7, 0), (1, 0, 1), (1, 0, 0), (0, 6, 1), (0, 2, 0),
    (0, 1, 1), (0, 1, 0), (1, 7, 1), (1, 7, 0), (0, 6, 0), (0, 3, 0), (0, 3, 1), (0, 5, 0),
    (0, 2, 1), (2, 0, 0), (1, 1, 0), (0, 4, 1), (0, 4, 0), (3, 0, 0), (1, 1, 1), (2, 7, 0),
    (0, 5, 1), (1, 3, 1), (1, 3, 0), (1, 6, 1), (1, 6, 0), (3, 7, 0), (1, 4, 0), (1, 4, 1),
    (2, 1, 0), (1, 5, 1), (1, 2, 1), (1, 5, 0), (1, 2, 0), (2, 3, 0), (4, 0, 0), (3, 1, 0),
    (4, 7, 0), (2, 6, 0), (2, 4, 0), (3, 3, 0), (4, 1, 0), (2, 5, 0), (3, 6, 0), (3, 4, 0),
    (4, 3, 0), (2, 2, 0), (3, 5, 0), (4, 6, 0), (4, 4, 0), (3, 2, 0), (4, 5, 0), (5, 3, 0),
    (4, 2, 0), (5, 3, 1), (5, 4, 1), (5, 4, 0), (5, 1, 0), (5, 7, 1), (5, 5, 1), (5, 5, 0),
    (5, 1, 1), (5, 7, 0), (5, 6, 1), (5, 2, 0), (5, 6, 0), (5, 2, 1), (5, 0, 1), (6, 4, 1),
    (6, 4, 0), (6, 3, 1), (5, 0, 0), (6, 3, 0), (6, 5, 1), (6, 5, 0), (6, 7, 0), (6, 6, 1),
    (6, 2, 0), (6, 2, 1), (6, 6, 0), (6, 0, 1), (6, 1, 1), (6, 1, 0), (6, 0, 0), (6, 7, 1),
)


def iota(shape, dim):
    return lax.broadcasted_iota(jnp.int32, shape, dim)


def kernel(
    tok_hbm, gain_hbm, ids_hbm, log_hbm, wg_hbm, wu_hbm, wd_hbm, out_ref,
    tok, gain, ids, logits, wg, wu, wd,
    own, ybuf, sbuf, xown, xoth, hown, hoth, ysend, r1buf, pacc, r2send, r2buf, r3send, r3buf,
    in_sem, w_sem, z_send, z_recv, s2_send, s2_recv, s3_send, s3_recv, x_send, x_recv,
    h_send, h_recv, r1_send, r1_recv, r2_send, r2_recv, r3_send, r3_recv,
):
    ep = lax.axis_index("ep")
    c = lax.axis_index("tp")
    x = lax.rem(ep, NX)
    y = lax.rem(ep // NX, NY)
    z = ep // (NX * NY)

    def at(dx=0, dy=0, dz=0):
        px = lax.rem(x + dx, NX)
        py = lax.rem(y + dy, NY)
        pz = lax.rem(z + dz, NZ)
        return ((pz * NY + py) * NX + px, c)

    partner = (ep, 1 - c)

    def peer(col, j):
        return at(dy=j) if col == 0 else at(dx=j)

    def far(col, j):
        return at(dx=j) if col == 0 else at(dy=j)

    def remote(src, dst, send, recv, device):
        return pltpu.make_async_remote_copy(
            src_ref=src, dst_ref=dst, send_sem=send, recv_sem=recv, device_id=device, device_id_type=MESH
        )

    def drain(ref, sem):
        pltpu.make_async_copy(ref, ref, sem).wait()

    small = [
        pltpu.make_async_copy(tok_hbm, tok, in_sem.at[0]),
        pltpu.make_async_copy(gain_hbm, gain, in_sem.at[1]),
        pltpu.make_async_copy(ids_hbm, ids, in_sem.at[2]),
        pltpu.make_async_copy(log_hbm, logits, in_sem.at[3]),
    ]
    for copy in small:
        copy.start()
    weights = []
    for i, (src, dst) in enumerate(((wg_hbm, wg), (wu_hbm, wu), (wd_hbm, wd))):
        for part in range(2):
            start = pl.multiple_of(lax.rem(c + part, 2) * 512, 512)
            weights.append(
                pltpu.make_async_copy(src.at[pl.ds(start, 512)], dst.at[pl.ds(part * 512, 512)], w_sem.at[i, part])
            )

    barrier = pltpu.get_barrier_semaphore()
    friends = [at(dz=k) for k in range(1, NZ)] + [at(dy=j) for j in range(1, NY)] + [at(dx=j) for j in range(1, NX)]
    friends.append(partner)
    for friend in friends:
        pl.semaphore_signal(barrier, inc=1, device_id=friend, device_id_type=MESH)

    for copy in small:
        copy.wait()
    for copy in weights:
        copy.start()

    full = tok[...].astype(F32)
    scale = lax.rsqrt(jnp.mean(full * full, axis=-1, keepdims=True) + EPS)
    mine = pl.ds(pl.multiple_of(c * 512, 512), 512)
    normed = (tok[:, mine].astype(F32) * scale * gain[:, mine]).astype(BF)

    lane4 = iota((BLK, 128), 1)
    spread = (lax.rem(lane4, BLK) == iota((BLK, 128), 0)).astype(BF)
    raw = logits[...]
    shifted = jnp.exp(raw - jnp.max(raw, axis=0, keepdims=True))
    probs = shifted / jnp.sum(shifted, axis=0, keepdims=True)
    ids_l = jnp.dot(ids[...].astype(F32).astype(BF), spread, preferred_element_type=F32)
    probs_l = jnp.dot(probs.astype(BF), spread, preferred_element_type=F32)
    row = iota((128, 128), 0)
    lane = iota((128, 128), 1)
    plane = lax.rem(z + row // 16, NZ)
    near = lax.rem(row, 4)
    group = lane // BLK
    route_b = lax.rem(row // 8, 2) == 0
    ex = lax.rem(x + jnp.where(route_b, near, group), NX)
    ey = lax.rem(y + jnp.where(route_b, group, near), NY)
    expert = (plane * 16 + ey * NX + ex).astype(F32)
    named = jnp.zeros((128, 128), F32)
    weight = jnp.zeros((128, 128), F32)
    for q in range(4):
        hit = expert == ids_l[q : q + 1, :]
        named = jnp.where(hit, 1.0, named)
        weight = jnp.where(hit, probs_l[q : q + 1, :], weight)
    before = ((row // BLK == lane // BLK) & (row < lane)).astype(BF)
    place = jnp.dot(named.astype(BF), before, preferred_element_type=F32)
    place = jnp.where(named > 0, place, -128.0)
    meta = jnp.where(lax.rem(row, 8) < 4, place, weight).astype(BF)
    blank = jnp.zeros((8, HALF - 128), BF)
    for k in range(NZ):
        for col in range(2):
            dst = own.at[k, col] if k else ybuf.at[0, col, 0]
            dst[:BLK, :] = normed[:, col * HALF : (col + 1) * HALF]
            dst[BLK:, :128] = meta[k * 16 + col * 8 : k * 16 + col * 8 + 8, :]
            dst[BLK:, 128:] = blank

    pl.semaphore_wait(barrier, len(friends))

    def start_z():
        for k in (1, 7, 2, 6, 3, 5, 4):
            slot = (-k) % NZ
            remote(own.at[k], ybuf.at[slot, :, 0], z_send, z_recv.at[slot], at(dz=k)).start()

    seen = set()

    def s2(k, col):
        if k and k not in seen:
            drain(own.at[k], z_recv.at[k])
            seen.add(k)
        for j in (1, 3, 2):
            remote(
                ybuf.at[k, col, 0], ybuf.at[k, col, (-j) % 4], s2_send, s2_recv.at[k, col], peer(col, j)
            ).start()

    lanes = iota((8, 128), 1) // BLK
    sixty = iota((64, 128), 0)
    base = (iota((1, 128), 1) // BLK * CAP).astype(F32)

    def table(k, col):
        t = [ybuf[k, col, s, BLK:, :128].astype(F32) for s in range(4)]
        t1 = pltpu.roll(t[1], 64, 1)
        t3 = pltpu.roll(t[3], 64, 1)
        return jnp.where(lanes == 0, t[0], jnp.where(lanes == 1, t1, jnp.where(lanes == 2, t[2], t3)))

    def select(k, col, weighted):
        m = table(k, col)
        parts = []
        for j in range(4):
            wanted = (m[j : j + 1, :] + base).astype(jnp.int32)
            value = m[4 + j : 5 + j, :] if weighted else 1.0
            parts.append(jnp.where(sixty == wanted, value, 0.0).astype(BF))
        return jnp.concatenate(parts, axis=0)

    def s3(k, col):
        drain(ybuf.at[k, col, pl.ds(1, 3)], s2_recv.at[k, col])
        rows = ybuf[k, col, :, :BLK, :].reshape(128, HALF)
        packed = jnp.dot(select(k, col, False), rows, preferred_element_type=F32).astype(BF)
        for j in range(4):
            piece = packed[64 * j : 64 * j + 64].reshape(4, CAP, HALF)
            if j:
                sbuf[k, col, j - 1] = piece
            elif col == 0:
                xown[k, 0, 0] = piece
            else:
                xown[k, 1, :, 0] = piece
        for j in (1, 3, 2):
            slot = (-j) % 4
            dst = xown.at[k, 0, slot] if col == 0 else xown.at[k, 1, :, slot]
            remote(sbuf.at[k, col, j - 1], dst, s3_send, s3_recv.at[k, col], far(col, j)).start()

    def x4(k, _):
        for col in range(2):
            drain(sbuf.at[k, col], s3_recv.at[k, col])
        remote(xown.at[k], xoth.at[k], x_send, x_recv.at[k], partner).start()

    def g5(k, _):
        if "w" not in seen:
            seen.add("w")
            for copy in weights:
                copy.wait()
        drain(xoth.at[k], x_recv.at[k])
        rows = jnp.concatenate([ref[k, col].reshape(256, HALF) for ref in (xown, xoth) for col in range(2)], axis=1)
        gate = jnp.minimum(jnp.dot(rows, wg[...], preferred_element_type=F32), 7.0)
        lin = jnp.clip(jnp.dot(rows, wu[...], preferred_element_type=F32), -7.0, 7.0)
        sig = 0.5 * jnp.tanh(0.851 * gate) + 0.5
        hown[k] = (gate * sig * (lin + 1.0)).astype(BF)
        remote(hown.at[k], hoth.at[k], h_send, h_recv.at[k], partner).start()

    def d6(k, _):
        drain(hoth.at[k], h_recv.at[k])
        hidden = jnp.concatenate([hown[k], hoth[k]], axis=1)
        done = jnp.dot(hidden, wd[...], preferred_element_type=F32).astype(BF)
        for col in range(2):
            rows = done[:, col * HALF : (col + 1) * HALF].reshape(4, 4, CAP, HALF)
            for j in range(4):
                piece = rows[j] if col == 0 else rows[:, j]
                if j:
                    ysend[k, col, j - 1] = piece
                else:
                    r1buf[k, col, 0] = piece
            for j in (1, 3, 2):
                remote(
                    ysend.at[k, col, j - 1], r1buf.at[k, col, (-j) % 4], r1_send, r1_recv.at[k, col], far(col, j)
                ).start()

    def u7(k, col):
        drain(ysend.at[k, col], r1_recv.at[k, col])
        rows = r1buf[k, col].reshape(256, HALF)
        sums = lax.dot_general(select(k, col, True), rows, (((0,), (0,)), ((), ())), preferred_element_type=F32)
        pacc[k, col] = sums[:BLK]
        for j in range(1, 4):
            r2send[k, col, j - 1] = sums[BLK * j : BLK * j + BLK].astype(BF)
        for j in (1, 3, 2):
            remote(
                r2send.at[k, col, j - 1], r2buf.at[k, col, (-j) % 4 - 1], r2_send, r2_recv.at[k, col], peer(col, j)
            ).start()

    def r8(k, col):
        drain(r2buf.at[k, col], r2_recv.at[k, col])
        total = pacc[k, col]
        for j in range(3):
            total = total + r2buf[k, col, j].astype(F32)
        if k:
            r3send[k, col] = total.astype(BF)
        else:
            pacc[0, col] = total
        if k and ("r", k) in seen:
            slot = (-k) % NZ
            remote(r3send.at[k], r3buf.at[slot], r3_send, r3_recv.at[slot], at(dz=k)).start()
        seen.add(("r", k))

    start_z()
    steps = (s2, s3, x4, g5, d6, u7, r8)
    for step, k, col in SEQ:
        steps[step](k, col)

    for col in range(2):
        total = pacc[0, col]
        for k in range(1, NZ):
            if col == 0:
                drain(r3buf.at[k], r3_recv.at[k])
            total = total + r3buf[k, col].astype(F32)
        out_ref[:, col * HALF : (col + 1) * HALF] = total.astype(BF)

    drain(own.at[pl.ds(1, 7)], z_send)
    drain(ybuf.at[:, :, pl.ds(1, 3)], s2_send)
    drain(sbuf, s3_send)
    drain(xown, x_send)
    drain(hown, h_send)
    drain(ysend, r1_send)
    drain(r2send, r2_send)
    drain(r3send.at[pl.ds(1, 7)], r3_send)


def shards(tokens, norm_gain, routing, route_logits, w_gate, w_up, w_down):
    vmem = pltpu.VMEM
    dma = pltpu.SemaphoreType.DMA
    return pl.pallas_call(
        kernel,
        name="routed_layer",
        out_shape=vmem((BLK, 2 * HALF), BF),
        in_specs=[pl.BlockSpec(memory_space=pl.ANY)] * 7,
        out_specs=pl.BlockSpec(memory_space=vmem),
        scratch_shapes=[
            vmem((BLK, 1024), BF),
            vmem((1, 1024), F32),
            vmem((4, BLK), jnp.int32),
            vmem((4, BLK), F32),
            vmem((1024, 512), BF),
            vmem((1024, 512), BF),
            vmem((1024, 512), BF),
            vmem((NZ, 2, ROWS, HALF), BF),
            vmem((NZ, 2, 4, ROWS, HALF), BF),
            vmem((NZ, 2, 3, 4, CAP, HALF), BF),
            vmem((NZ, 2, 4, 4, CAP, HALF), BF),
            vmem((NZ, 2, 4, 4, CAP, HALF), BF),
            vmem((NZ, 256, 512), BF),
            vmem((NZ, 256, 512), BF),
            vmem((NZ, 2, 3, 4, CAP, HALF), BF),
            vmem((NZ, 2, 4, 4, CAP, HALF), BF),
            vmem((NZ, 2, BLK, HALF), F32),
            vmem((NZ, 2, 3, BLK, HALF), BF),
            vmem((NZ, 2, 3, BLK, HALF), BF),
            vmem((NZ, 2, BLK, HALF), BF),
            vmem((NZ, 2, BLK, HALF), BF),
            dma((4,)),
            dma((3, 2)),
            dma, dma((NZ,)),
            dma, dma((NZ, 2)),
            dma, dma((NZ, 2)),
            dma, dma((NZ,)),
            dma, dma((NZ,)),
            dma, dma((NZ, 2)),
            dma, dma((NZ, 2)),
            dma, dma((NZ,)),
        ],
        compiler_params=pltpu.CompilerParams(
            collective_id=0, has_side_effects=True, vmem_limit_bytes=60 * 1024 * 1024
        ),
    )(tokens, norm_gain.reshape(1, -1), routing.T, route_logits.T, w_gate[0], w_up[0], w_down[0])


def solution(mesh):
    return jax.shard_map(
        shards,
        mesh=mesh,
        in_specs=(
            P("ep", None),
            P(),
            P("ep", None),
            P("ep", None),
            P("ep", None, "tp"),
            P("ep", None, "tp"),
            P("ep", None, "tp"),
        ),
        out_specs=P("ep", "tp"),
        check_vma=False,
    )
```

```python
import jax
import jax.numpy as jnp
from jax import lax
from jax.experimental import pallas as pl
from jax.experimental.pallas import tpu as pltpu
from jax.sharding import PartitionSpec as P

MESH = pl.DeviceIdType.MESH
NX, NY, NZ = 4, 4, 8
CAP = 16
BLK = 32
HALF = 256
EPS = 1e-05
BF = jnp.bfloat16
F32 = jnp.float32
PAIRS = ((1, 7), (0, 2), (6, 3), (5, 4))
NEAR = (1, 7)
DISTANT = (2, 6, 3, 5, 4)
OWNER = {k: c for pair in PAIRS for c, k in enumerate(pair)}
PLACE = {k: i for i, pair in enumerate(PAIRS) for k in pair}
SEQ = (
    (0, 0, 0), (2, 7, 1), (2, 1, 0), (2, 1, 1), (2, 0, 1), (2, 0, 0), (1, 6, 1), (1, 5, 0),
    (1, 5, 1), (1, 4, 1), (1, 4, 0), (1, 3, 0), (2, 7, 0), (1, 6, 0), (1, 2, 1), (2, 6, 1),
    (1, 2, 0), (1, 3, 1), (2, 5, 0), (2, 5, 1), (2, 4, 0), (2, 6, 0), (2, 4, 1), (2, 3, 0),
    (2, 2, 1), (3, 0, 0), (2, 3, 1), (3, 0, 1), (2, 2, 0), (4, 0, 0), (4, 0, 1), (3, 3, 0),
    (3, 3, 1), (4, 3, 1), (4, 3, 0), (3, 2, 0), (3, 2, 1), (4, 2, 1), (4, 2, 0), (3, 1, 0),
    (3, 1, 1), (5, 4, 1), (5, 4, 0), (4, 1, 0), (5, 5, 1), (4, 1, 1), (5, 3, 0), (5, 3, 1),
    (5, 5, 0), (6, 4, 1), (5, 6, 1), (5, 6, 0), (6, 4, 0), (5, 1, 0), (5, 2, 1), (5, 2, 0),
    (6, 5, 1), (6, 3, 0), (5, 1, 1), (6, 5, 0), (6, 3, 1), (5, 7, 0), (5, 0, 0), (5, 0, 1),
    (6, 6, 1), (6, 6, 0), (7, 0, 0), (5, 7, 1), (7, 0, 1), (6, 2, 0), (6, 2, 1),
)


def iota(shape, dim):
    return lax.broadcasted_iota(jnp.int32, shape, dim)


def kernel(
    tok_hbm, gain_hbm, ids_hbm, log_hbm, wg_hbm, wu_hbm, wd_hbm, out_ref,
    tok, gain, ids, logits, wg, wu, wd,
    lsend, lmeta, msrc, mtab, pbuf, sbuf, xbuf, hid, ysend, r1buf, eacc, pacc, r2send, r2buf, r3send, r3buf,
    in_sem, w_sem, w_send, w_recv, l_send, l_recv, m_send, m_recv, z_send, z_recv, s2_send, s2_recv,
    s3_send, x_recv, r1_send, r1_recv, r1_own, r2_send, r2_recv, r3_send, r3_recv,
):
    ep = lax.axis_index("ep")
    c = lax.axis_index("tp")
    x = lax.rem(ep, NX)
    y = lax.rem(ep // NX, NY)
    z = ep // (NX * NY)

    def at(dx=0, dy=0, dz=0, core=None):
        px = lax.rem(x + dx, NX)
        py = lax.rem(y + dy, NY)
        pz = lax.rem(z + dz, NZ)
        return ((pz * NY + py) * NX + px, c if core is None else core)

    partner = (ep, 1 - c)

    def peer(col, j):
        return at(dy=j) if col == 0 else at(dx=j)

    def far(col, j, dz, core):
        return at(dx=j, dz=dz, core=core) if col == 0 else at(dy=j, dz=dz, core=core)

    def remote(src, dst, send, recv, device):
        pltpu.make_async_remote_copy(
            src_ref=src, dst_ref=dst, send_sem=send, recv_sem=recv, device_id=device, device_id_type=MESH
        ).start()

    def drain(ref, sem):
        pltpu.make_async_copy(ref, ref, sem).wait()

    small = [
        pltpu.make_async_copy(tok_hbm, tok, in_sem.at[0]),
        pltpu.make_async_copy(gain_hbm, gain, in_sem.at[1]),
        pltpu.make_async_copy(ids_hbm, ids, in_sem.at[2]),
        pltpu.make_async_copy(log_hbm, logits, in_sem.at[3]),
    ]
    for copy in small:
        copy.start()

    barrier = pltpu.get_barrier_semaphore()
    both = (0, 1)
    friends = [partner]
    friends += [at(dy=j, core=o) for j in range(1, NY) for o in both]
    friends += [at(dx=j, core=o) for j in range(1, NX) for o in both]
    for k in NEAR:
        friends += [at(dz=k, core=o) for o in both]
        friends += [at(dy=j, dz=k, core=o) for j in range(1, NY) for o in both]
        friends += [at(dx=j, dz=k, core=o) for j in range(1, NX) for o in both]
    friends += [at(dz=k) for k in DISTANT]
    for friend in friends:
        pl.semaphore_signal(barrier, inc=1, device_id=friend, device_id_type=MESH)

    for copy in small:
        copy.wait()
    weights = [pltpu.make_async_copy(src, dst.at[c], w_sem.at[i]) for i, (src, dst) in enumerate(((wg_hbm, wg), (wu_hbm, wu), (wd_hbm, wd)))]
    for copy in weights:
        copy.start()

    full = tok[...].astype(F32)
    scale = lax.rsqrt(jnp.mean(full * full, axis=-1, keepdims=True) + EPS)
    mine = pl.ds(pl.multiple_of(c * 512, 512), 512)
    normed = (tok[:, mine].astype(F32) * scale * gain[:, mine]).astype(BF)
    for col in range(2):
        pbuf[0, col, 0] = normed[:, col * HALF : (col + 1) * HALF]

    spread = (lax.rem(iota((BLK, 128), 1), BLK) == iota((BLK, 128), 0)).astype(BF)
    raw = logits[...]
    shifted = jnp.exp(raw - jnp.max(raw, axis=0, keepdims=True))
    probs = shifted / jnp.sum(shifted, axis=0, keepdims=True)
    ids_l = jnp.dot(ids[...].astype(F32).astype(BF), spread, preferred_element_type=F32)
    probs_l = jnp.dot(probs.astype(BF), spread, preferred_element_type=F32)
    row = iota((128, 128), 0)
    lane = iota((128, 128), 1)
    plane = lax.rem(z + lax.rem(row // 8, 2) * 4 + lane // BLK, NZ)
    group = lax.rem(row // 16, 4)
    near = lax.rem(row, 4)
    route_b = row < 64
    ex = lax.rem(x + jnp.where(route_b, near, group), NX)
    ey = lax.rem(y + jnp.where(route_b, group, near), NY)
    expert = (plane * 16 + ey * NX + ex).astype(F32)
    named = jnp.zeros((128, 128), F32)
    weight = jnp.zeros((128, 128), F32)
    for q in range(4):
        hit = expert == ids_l[q : q + 1, :]
        named = jnp.where(hit, 1.0, named)
        weight = jnp.where(hit, probs_l[q : q + 1, :], weight)
    before = ((row // BLK == lane // BLK) & (row < lane)).astype(BF)
    place = jnp.dot(named.astype(BF), before, preferred_element_type=F32)
    place = jnp.where(named > 0, place, -128.0)
    meta = jnp.where(lax.rem(row, 8) < 4, place, weight).astype(BF)
    for col in range(2):
        for g in range(4):
            for hi in range(2):
                start = col * 64 + g * 16 + hi * 8
                tile = meta[start : start + 8, :]
                if g:
                    lsend[col, g, hi] = tile
                else:
                    lmeta[col, 0, hi] = tile

    pl.semaphore_wait(barrier, len(friends))

    for col in range(2):
        for j in (1, 3, 2):
            remote(lsend.at[col, j], lmeta.at[col, (-j) % 4], l_send, l_recv.at[col], peer(col, j))
            remote(pbuf.at[0, col, 0], pbuf.at[0, col, (-j) % 4], s2_send, s2_recv.at[0, col], peer(col, j))
    for k in DISTANT:
        slot = (-k) % NZ
        remote(pbuf.at[0, :, 0], pbuf.at[slot, :, 0], z_send, z_recv.at[slot], at(dz=k))
    for i, (src, dst) in enumerate(((wg_hbm, wg), (wu_hbm, wu), (wd_hbm, wd))):
        remote(src, dst.at[c], w_send, w_recv.at[i], partner)

    seen = set()

    def once(key):
        if key in seen:
            return False
        seen.add(key)
        return True

    def mb(k, col):
        lanes = iota((8, 128), 1) // BLK
        base = jnp.where(iota((8, 128), 0) < 4, lanes * CAP, 0).astype(F32)
        for col in range(2):
            drain(lsend.at[col, pl.ds(1, 3)], l_recv.at[col])
            for hi in range(2):
                t = [lmeta[col, s, hi].astype(F32) for s in range(4)]
                for lo in range(4):
                    turned = [t[s] if s == lo else pltpu.roll(t[s], BLK * ((s - lo) % 4), 1) for s in range(4)]
                    m = jnp.where(
                        lanes < 2, jnp.where(lanes == 0, turned[0], turned[1]), jnp.where(lanes == 2, turned[2], turned[3])
                    )
                    msrc[hi * 4 + lo, col] = (m + base).astype(BF)
        for k in DISTANT:
            slot = (-k) % NZ
            remote(msrc.at[k], mtab.at[slot], m_send, m_recv.at[slot], at(dz=k))

    def s2(k, col):
        if once(("z", k)):
            drain(pbuf.at[k, :, 0], z_recv.at[k])
        for j in (1, 3, 2):
            remote(pbuf.at[k, col, 0], pbuf.at[k, col, (-j) % 4], s2_send, s2_recv.at[k, col], peer(col, j))

    def table(k, col):
        if k == 0 or k in NEAR:
            return msrc[k, col].astype(F32)
        return mtab[k, col].astype(F32)

    def select(k, col, weighted):
        m = table(k, col)
        sixty = iota((64, 128), 0).astype(F32)
        parts = []
        for j in range(4):
            value = m[4 + j : 5 + j, :] if weighted else 1.0
            parts.append(jnp.where(sixty == m[j : j + 1, :], value, 0.0).astype(BF))
        return jnp.concatenate(parts, axis=0)

    def s3(k, col):
        source = 0 if k in NEAR else k
        if once(("s2", source, col)):
            drain(pbuf.at[source, col, pl.ds(1, 3)], s2_recv.at[source, col])
        if k in DISTANT and once(("m", k)):
            drain(mtab.at[k], m_recv.at[k])
        rows = pbuf[source, col].reshape(128, HALF)
        packed = jnp.dot(select(k, col, False), rows, preferred_element_type=F32).astype(BF)
        there = (-k) % NZ if k in NEAR else k
        i, core = PLACE[there], OWNER[there]

        def target(slot):
            return xbuf.at[i, c, 0, slot] if col == 0 else xbuf.at[i, c, 1, :, slot]

        pieces = [packed[64 * j : 64 * j + 64].reshape(4, CAP, HALF) for j in range(4)]
        for j in range(4):
            if j or k in NEAR:
                sbuf[k, col, j] = pieces[j]
        for j in (1, 3, 2, 0) if k in NEAR else (1, 3, 2):
            device = far(col, j, k if k in NEAR else 0, core)
            remote(sbuf.at[k, col, j], target((-j) % 4), s3_send.at[1 if k in NEAR else 0], x_recv.at[i, c, col], device)
        if k not in NEAR:

            @pl.when(c == core)
            def _():
                if col == 0:
                    xbuf[i, c, 0, 0] = pieces[0]
                else:
                    xbuf[i, c, 1, :, 0] = pieces[0]

            @pl.when(c != core)
            def _():
                sbuf[k, col, 0] = pieces[0]
                remote(sbuf.at[k, col, 0], target(0), s3_send.at[2], x_recv.at[i, c, col], partner)

    def ga(i, h):
        if once(("x", i)):
            for col in range(2):
                if PAIRS[i][0] in NEAR:
                    drain(sbuf.at[0, 0], x_recv.at[i, c, col])
                else:
                    drain(sbuf.at[0, 0, pl.ds(1, 3)], x_recv.at[i, c, col])
                drain(sbuf.at[0, 0], x_recv.at[i, 1 - c, col])
        if once("w"):
            for n in range(2):
                weights[n].wait()
                drain(wg.at[0], w_recv.at[n])
        rows = jnp.concatenate([xbuf[i, s, col].reshape(256, HALF) for s in range(2) for col in range(2)], axis=1)
        gate = jnp.minimum(jnp.dot(rows, wg[h], preferred_element_type=F32), 7.0)
        lin = jnp.clip(jnp.dot(rows, wu[h], preferred_element_type=F32), -7.0, 7.0)
        sig = 0.5 * jnp.tanh(0.851 * gate) + 0.5
        hid[i, h] = (gate * sig * (lin + 1.0)).astype(BF)

    def db(i, h):
        if once("d"):
            weights[2].wait()
            drain(wd.at[0], w_recv.at[2])
        hidden = jnp.concatenate([hid[i, 0], hid[i, 1]], axis=1)
        done = jnp.dot(hidden, wd[h], preferred_element_type=F32).astype(BF)
        k0, k1 = PAIRS[i]
        close = k0 in NEAR
        k = k0 + c * (k1 - k0)
        there = lax.rem(NZ - k, NZ) if close else k
        for col in range(2):
            rows = done[:, col * HALF : (col + 1) * HALF].reshape(4, 4, CAP, HALF)
            pieces = [rows[j] if col == 0 else rows[:, j] for j in range(4)]
            for j in range(4):
                if j or close:
                    ysend[i, h, col, j] = pieces[j]
            for j in (1, 3, 2, 0) if close else (1, 3, 2):
                device = far(col, j, k if close else 0, h)
                remote(
                    ysend.at[i, h, col, j], r1buf.at[there, col, (-j) % 4], r1_send.at[1 if close else 0],
                    r1_recv.at[there, col], device,
                )
            if not close:

                @pl.when(c == h)
                def _():
                    r1buf[there, col, 0] = pieces[0]

                @pl.when(c != h)
                def _():
                    ysend[i, h, col, 0] = pieces[0]
                    remote(
                        ysend.at[i, h, col, 0], r1buf.at[there, col, 0], r1_send.at[2], r1_own.at[there, col], partner
                    )

    def to_line(k, col, sums):
        pacc[k, col] = sums[:BLK]
        for j in range(1, 4):
            r2send[k, col, j - 1] = sums[BLK * j : BLK * j + BLK].astype(BF)
        for j in (1, 3, 2):
            remote(
                r2send.at[k, col, j - 1], r2buf.at[k, col, (-j) % 4 - 1], r2_send.at[1 if k else 0],
                r2_recv.at[k, col], peer(col, j),
            )

    def u7(k, col):
        if k in NEAR:
            drain(ysend.at[0, 0, 0], r1_recv.at[k, col])
        else:
            drain(ysend.at[0, 0, 0, pl.ds(1, 3)], r1_recv.at[k, col])

            @pl.when(c != OWNER[k])
            def _():
                drain(ysend.at[0, 0, 0, 0], r1_own.at[k, col])

        rows = r1buf[k, col].reshape(256, HALF)
        sums = lax.dot_general(select(k, col, True), rows, (((0,), (0,)), ((), ())), preferred_element_type=F32)
        if k == 0 or k in NEAR:
            if once(("e", col)):
                eacc[col] = sums
            else:
                eacc[col] += sums
        else:
            to_line(k, col, sums)

    def e2(k, col):
        to_line(0, col, eacc[col])

    def r8(k, col):
        drain(r2buf.at[k, col], r2_recv.at[k, col])
        total = pacc[k, col]
        for j in range(3):
            total = total + r2buf[k, col, j].astype(F32)
        slot = (-k) % NZ
        r3send[k, col] = total.astype(BF)
        remote(r3send.at[k, col], r3buf.at[slot, col], r3_send, r3_recv.at[slot, col], at(dz=k))

    steps = (mb, s2, s3, ga, db, u7, r8, e2)
    for step, k, col in SEQ:
        pl.when(c < 2)(lambda step=step, k=k, col=col: steps[step](k, col))

    for col in range(2):
        total = pacc[0, col]
        for k in DISTANT:
            drain(r3buf.at[k, col], r3_recv.at[k, col])
            total = total + r3buf[k, col].astype(F32)
        drain(r2buf.at[0, col], r2_recv.at[0, col])
        for j in range(3):
            total = total + r2buf[0, col, j].astype(F32)
        out_ref[:, col * HALF : (col + 1) * HALF] = total.astype(BF)

    six = pl.ds(0, 6)
    five = pl.ds(0, 5)
    three = pl.ds(0, 3)
    rest = pl.ds(1, 3)
    drain(lsend.at[:, rest], l_send)
    drain(pbuf.at[five, :, 0], z_send)
    drain(wg.at[0], w_send)
    drain(wu.at[0], w_send)
    drain(wd.at[0], w_send)
    drain(msrc.at[five], m_send)
    drain(pbuf.at[six, :, rest], s2_send)
    drain(sbuf.at[six, :, rest], s3_send.at[0])
    drain(sbuf.at[pl.ds(0, 2)], s3_send.at[1])
    drain(sbuf.at[three, :, 0], s3_send.at[2])
    drain(ysend.at[three, :, :, rest], r1_send.at[0])
    drain(ysend.at[0], r1_send.at[1])
    drain(ysend.at[three, 0, :, 0], r1_send.at[2])
    drain(r2send.at[0], r2_send.at[0])
    drain(r2send.at[five], r2_send.at[1])
    drain(r3send.at[five], r3_send)


def shards(tokens, norm_gain, routing, route_logits, w_gate, w_up, w_down):
    vmem = pltpu.VMEM
    dma = pltpu.SemaphoreType.DMA
    return pl.pallas_call(
        kernel,
        name="routed_layer",
        out_shape=vmem((BLK, 2 * HALF), BF),
        in_specs=[pl.BlockSpec(memory_space=pl.ANY)] * 7,
        out_specs=pl.BlockSpec(memory_space=vmem),
        scratch_shapes=[
            vmem((BLK, 1024), BF),
            vmem((1, 1024), F32),
            vmem((4, BLK), jnp.int32),
            vmem((4, BLK), F32),
            vmem((2, 1024, 512), BF),
            vmem((2, 1024, 512), BF),
            vmem((2, 1024, 512), BF),
            vmem((2, 4, 2, 8, 128), BF),
            vmem((2, 4, 2, 8, 128), BF),
            vmem((NZ, 2, 8, 128), BF),
            vmem((NZ, 2, 8, 128), BF),
            vmem((NZ, 2, 4, BLK, HALF), BF),
            vmem((NZ, 2, 4, 4, CAP, HALF), BF),
            vmem((4, 2, 2, 4, 4, CAP, HALF), BF),
            vmem((4, 2, 256, 512), BF),
            vmem((4, 2, 2, 4, 4, CAP, HALF), BF),
            vmem((NZ, 2, 4, 4, CAP, HALF), BF),
            vmem((2, 128, HALF), F32),
            vmem((NZ, 2, BLK, HALF), F32),
            vmem((NZ, 2, 3, BLK, HALF), BF),
            vmem((NZ, 2, 3, BLK, HALF), BF),
            vmem((NZ, 2, BLK, HALF), BF),
            vmem((NZ, 2, BLK, HALF), BF),
            dma((4,)),
            dma((3,)),
            dma, dma((3,)),
            dma, dma((2,)),
            dma, dma((NZ,)),
            dma, dma((NZ,)),
            dma, dma((NZ, 2)),
            dma((3,)), dma((4, 2, 2)),
            dma((3,)), dma((NZ, 2)), dma((NZ, 2)),
            dma((2,)), dma((NZ, 2)),
            dma, dma((NZ, 2)),
        ],
        compiler_params=pltpu.CompilerParams(
            collective_id=0, has_side_effects=True, vmem_limit_bytes=60 * 1024 * 1024
        ),
    )(tokens, norm_gain.reshape(1, -1), routing.T, route_logits.T, w_gate[0], w_up[0], w_down[0])


def solution(mesh):
    return jax.shard_map(
        shards,
        mesh=mesh,
        in_specs=(
            P("ep", None),
            P(),
            P("ep", None),
            P("ep", None),
            P("ep", None, "tp"),
            P("ep", None, "tp"),
            P("ep", None, "tp"),
        ),
        out_specs=P("ep", "tp"),
        check_vma=False,
    )
```

```python
import jax
import jax.numpy as jnp
from jax import lax
from jax.experimental import pallas as pl
from jax.experimental.pallas import tpu as pltpu
from jax.sharding import PartitionSpec as P

MESH = pl.DeviceIdType.MESH
NX, NY, NZ = 4, 4, 8
CAP = 16
BLK = 32
HALF = 256
EPS = 1e-05
BF = jnp.bfloat16
F32 = jnp.float32
PAIRS = ((1, 0), (7, 2), (6, 3), (5, 4))
NEAR = ()
DISTANT = tuple(k for k in (1, 7, 2, 6, 3, 5, 4) if k not in NEAR)
NFAR = len(DISTANT)
BUNDLE = (3, 5)
SINGLE = tuple(k for k in DISTANT if k not in BUNDLE)
FAR = {k: n for n, k in enumerate(DISTANT)}
LINED = {k: n for n, k in enumerate((0,) + DISTANT)}
ALONE = {k: n for n, k in enumerate((0,) + SINGLE)}
OWNER = {k: c for pair in PAIRS for c, k in enumerate(pair)}
PLACE = {k: i for i, pair in enumerate(PAIRS) for k in pair}
SEQ = (
    (1, 7, 1), (1, 1, 1), (1, 1, 0), (0, 0, 0), (1, 7, 0), (8, 0, 1), (1, 2, 1), (1, 2, 0),
    (2, 0, 1), (8, 0, 0), (1, 6, 0), (2, 0, 0), (2, 7, 1), (1, 6, 1), (2, 7, 0), (1, 4, 1),
    (1, 4, 0), (2, 1, 0), (2, 2, 1), (2, 1, 1), (2, 2, 0), (2, 6, 0), (2, 4, 1), (2, 5, 1),
    (2, 3, 1), (2, 4, 0), (2, 5, 0), (2, 6, 1), (3, 0, 0), (2, 3, 0), (3, 1, 0), (3, 1, 1),
    (4, 1, 1), (4, 1, 0), (3, 3, 0), (3, 3, 1), (4, 3, 1), (4, 3, 0), (3, 2, 0), (3, 2, 1),
    (4, 2, 0), (3, 0, 1), (5, 4, 0), (5, 4, 1), (4, 0, 0), (4, 2, 1), (5, 3, 1), (5, 5, 0),
    (5, 5, 1), (5, 2, 1), (5, 3, 0), (4, 0, 1), (5, 6, 0), (5, 2, 0), (5, 7, 0), (6, 4, 1),
    (5, 6, 1), (6, 4, 0), (5, 7, 1), (6, 5, 0), (5, 1, 1), (6, 3, 1), (6, 3, 0), (6, 5, 1),
    (5, 1, 0), (6, 2, 1), (5, 0, 0), (7, 0, 0), (6, 6, 0), (5, 0, 1), (7, 0, 1), (6, 6, 1),
    (6, 2, 0), (6, 7, 0), (6, 7, 1), (6, 1, 1), (6, 1, 0),
)


def iota(shape, dim):
    return lax.broadcasted_iota(jnp.int32, shape, dim)


def kernel(
    tok_hbm, gain_hbm, ids_hbm, log_hbm, wg_hbm, wu_hbm, wd_hbm, out_ref,
    tok, gain, ids, logits, wg, wu, wd,
    lsend, lmeta, msrc, mtab, pbuf, sbuf, xbuf, hid, ysend, r1buf, eacc, pacc, r2send, r2buf, r3send, r3buf,
    in_sem, w_sem, w_recv, sent, l_recv, m_recv, z_recv, b_recv, s2_recv, x_recv, r1_recv, r2_recv, r3_recv,
):
    ep = lax.axis_index("ep")
    c = lax.axis_index("tp")
    x = lax.rem(ep, NX)
    y = lax.rem(ep // NX, NY)
    z = ep // (NX * NY)

    def at(dx=0, dy=0, dz=0, core=None):
        px = lax.rem(x + dx, NX)
        py = lax.rem(y + dy, NY)
        pz = lax.rem(z + dz, NZ)
        return ((pz * NY + py) * NX + px, c if core is None else core)

    partner = (ep, 1 - c)

    def peer(col, j):
        return at(dy=j) if col == 0 else at(dx=j)

    def far(col, j, dz, core):
        return at(dx=j, dz=dz, core=core) if col == 0 else at(dy=j, dz=dz, core=core)

    def remote(src, dst, send, recv, device):
        pltpu.make_async_remote_copy(
            src_ref=src, dst_ref=dst, send_sem=send, recv_sem=recv, device_id=device, device_id_type=MESH
        ).start()

    def drain(ref, sem):
        pltpu.make_async_copy(ref, ref, sem).wait()

    small = [
        pltpu.make_async_copy(tok_hbm, tok, in_sem.at[0]),
        pltpu.make_async_copy(gain_hbm, gain, in_sem.at[1]),
        pltpu.make_async_copy(ids_hbm, ids, in_sem.at[2]),
        pltpu.make_async_copy(log_hbm, logits, in_sem.at[3]),
    ]
    for copy in small:
        copy.start()

    barrier = pltpu.get_barrier_semaphore()
    both = (0, 1)
    friends = [partner]
    friends += [at(dy=j, core=o) for j in range(1, NY) for o in both]
    friends += [at(dx=j, core=o) for j in range(1, NX) for o in both]
    for k in NEAR:
        friends += [at(dz=k, core=o) for o in both]
        friends += [at(dy=j, dz=k, core=o) for j in range(1, NY) for o in both]
        friends += [at(dx=j, dz=k, core=o) for j in range(1, NX) for o in both]
    friends += [at(dz=k) for k in DISTANT]
    for friend in friends:
        pl.semaphore_signal(barrier, inc=1, device_id=friend, device_id_type=MESH)

    for copy in small:
        copy.wait()
    weights = ((wg_hbm, wg, 0), (wu_hbm, wu, 0), (wd_hbm, wd, 1))
    for src, dst, n in weights:
        pltpu.make_async_copy(src, dst.at[c], w_sem.at[n]).start()

    full = tok[...].astype(F32)
    scale = lax.rsqrt(jnp.mean(full * full, axis=-1, keepdims=True) + EPS)
    mine = pl.ds(pl.multiple_of(c * 512, 512), 512)
    normed = (tok[:, mine].astype(F32) * scale * gain[:, mine]).astype(BF)
    for col in range(2):
        pbuf[0, col, 0] = normed[:, col * HALF : (col + 1) * HALF]

    spread = (lax.rem(iota((BLK, 128), 1), BLK) == iota((BLK, 128), 0)).astype(BF)
    raw = logits[...]
    shifted = jnp.exp(raw - jnp.max(raw, axis=0, keepdims=True))
    probs = shifted / jnp.sum(shifted, axis=0, keepdims=True)
    ids_l = jnp.dot(ids[...].astype(F32).astype(BF), spread, preferred_element_type=F32)
    probs_l = jnp.dot(probs.astype(BF), spread, preferred_element_type=F32)
    row = iota((128, 128), 0)
    lane = iota((128, 128), 1)
    plane = lax.rem(z + lax.rem(row // 8, 2) * 4 + lane // BLK, NZ)
    group = lax.rem(row // 16, 4)
    near = lax.rem(row, 4)
    route_b = row < 64
    ex = lax.rem(x + jnp.where(route_b, near, group), NX)
    ey = lax.rem(y + jnp.where(route_b, group, near), NY)
    expert = (plane * 16 + ey * NX + ex).astype(F32)
    named = jnp.zeros((128, 128), F32)
    weight = jnp.zeros((128, 128), F32)
    for q in range(4):
        hit = expert == ids_l[q : q + 1, :]
        named = jnp.where(hit, 1.0, named)
        weight = jnp.where(hit, probs_l[q : q + 1, :], weight)
    before = ((row // BLK == lane // BLK) & (row < lane)).astype(BF)
    place = jnp.dot(named.astype(BF), before, preferred_element_type=F32)
    place = jnp.where(named > 0, place, -128.0)
    meta = jnp.where(lax.rem(row, 8) < 4, place, weight).astype(BF)
    for col in range(2):
        for g in range(4):
            for hi in range(2):
                start = col * 64 + g * 16 + hi * 8
                tile = meta[start : start + 8, :]
                if g:
                    lsend[col, g, hi] = tile
                else:
                    lmeta[col, 0, hi] = tile

    pl.semaphore_wait(barrier, len(friends))

    for col in range(2):
        for j in (1, 3, 2):
            remote(lsend.at[col, j], lmeta.at[col, (-j) % 4], sent, l_recv, peer(col, j))
            remote(pbuf.at[0, col, 0], pbuf.at[0, col, (-j) % 4], sent, s2_recv.at[0, col], peer(col, j))
    for k in SINGLE:
        slot = (-k) % NZ
        remote(pbuf.at[0, :, 0], pbuf.at[slot, :, 0], sent, z_recv.at[ALONE[slot]], at(dz=k))
    for src, dst, n in weights:
        remote(src, dst.at[c], sent, w_recv.at[n], partner)

    seen = set()

    def once(key):
        if key in seen:
            return False
        seen.add(key)
        return True

    def mb(k, col):
        lanes = iota((8, 128), 1) // BLK
        base = jnp.where(iota((8, 128), 0) < 4, lanes * CAP, 0).astype(F32)
        drain(lsend.at[:, pl.ds(1, 3)], l_recv)
        for col in range(2):
            for hi in range(2):
                t = [lmeta[col, s, hi].astype(F32) for s in range(4)]
                for lo in range(4):
                    turned = [t[s] if s == lo else pltpu.roll(t[s], BLK * ((s - lo) % 4), 1) for s in range(4)]
                    m = jnp.where(
                        lanes < 2, jnp.where(lanes == 0, turned[0], turned[1]), jnp.where(lanes == 2, turned[2], turned[3])
                    )
                    msrc[hi * 4 + lo, col] = (m + base).astype(BF)
        for k in DISTANT:
            slot = (-k) % NZ
            remote(msrc.at[k], mtab.at[slot], sent, m_recv.at[FAR[slot]], at(dz=k))

    def s2(k, col):
        if once(("z", k)):
            drain(pbuf.at[k, :, 0], z_recv.at[ALONE[k]])
        for j in (1, 3, 2):
            remote(pbuf.at[k, col, 0], pbuf.at[k, col, (-j) % 4], sent, s2_recv.at[ALONE[k], col], peer(col, j))

    def table(k, col):
        if k == 0 or k in NEAR:
            return msrc[k, col].astype(F32)
        return mtab[k, col].astype(F32)

    def select(k, col, weighted):
        m = table(k, col)
        sixty = iota((64, 128), 0).astype(F32)
        parts = []
        for j in range(4):
            value = m[4 + j : 5 + j, :] if weighted else 1.0
            parts.append(jnp.where(sixty == m[j : j + 1, :], value, 0.0).astype(BF))
        return jnp.concatenate(parts, axis=0)

    def lined(k, col):
        if once(("s2", k, col)):
            if k in BUNDLE:
                drain(pbuf.at[k, col], b_recv.at[BUNDLE.index(k), col])
            else:
                drain(pbuf.at[k, col, pl.ds(1, 3)], s2_recv.at[ALONE[k], col])

    def zb(k, col):
        lined(0, col)
        for k in BUNDLE:
            slot = (-k) % NZ
            remote(pbuf.at[0, col], pbuf.at[slot, col], sent, b_recv.at[BUNDLE.index(slot), col], at(dz=k))

    def s3(k, col):
        source = 0 if k in NEAR else k
        lined(source, col)
        if k in DISTANT and once(("m", k)):
            drain(mtab.at[k], m_recv.at[FAR[k]])
        rows = pbuf[source, col].reshape(128, HALF)
        packed = jnp.dot(select(k, col, False), rows, preferred_element_type=F32).astype(BF)
        there = (-k) % NZ if k in NEAR else k
        i, core = PLACE[there], OWNER[there]

        def target(slot):
            return xbuf.at[i, c, 0, slot] if col == 0 else xbuf.at[i, c, 1, :, slot]

        pieces = [packed[64 * j : 64 * j + 64].reshape(4, CAP, HALF) for j in range(4)]
        for j in range(4):
            if j or k in NEAR:
                sbuf[k, col, j] = pieces[j]
        for j in (1, 3, 2, 0) if k in NEAR else (1, 3, 2):
            device = far(col, j, k if k in NEAR else 0, core)
            remote(sbuf.at[k, col, j], target((-j) % 4), sent, x_recv.at[i, c], device)
        if k not in NEAR:

            @pl.when(c == core)
            def _():
                if col == 0:
                    xbuf[i, c, 0, 0] = pieces[0]
                else:
                    xbuf[i, c, 1, :, 0] = pieces[0]

            @pl.when(c != core)
            def _():
                sbuf[k, col, 0] = pieces[0]
                remote(sbuf.at[k, col, 0], target(0), sent, x_recv.at[i, c], partner)

    def ga(i, h):
        if once(("x", i)):
            drain(sbuf.at[0] if PAIRS[i][0] in NEAR else sbuf.at[0, :, pl.ds(1, 3)], x_recv.at[i, c])
            drain(sbuf.at[0], x_recv.at[i, 1 - c])
        if once("w"):
            drain(wg, w_sem.at[0])
            drain(wg, w_recv.at[0])
        rows = jnp.concatenate([xbuf[i, s, col].reshape(256, HALF) for s in range(2) for col in range(2)], axis=1)
        gate = jnp.minimum(jnp.dot(rows, wg[h], preferred_element_type=F32), 7.0)
        lin = jnp.clip(jnp.dot(rows, wu[h], preferred_element_type=F32), -7.0, 7.0)
        sig = 0.5 * jnp.tanh(0.851 * gate) + 0.5
        hid[i, h] = (gate * sig * (lin + 1.0)).astype(BF)

    def db(i, h):
        if once("d"):
            drain(wd.at[0], w_sem.at[1])
            drain(wd.at[0], w_recv.at[1])
        hidden = jnp.concatenate([hid[i, 0], hid[i, 1]], axis=1)
        done = jnp.dot(hidden, wd[h], preferred_element_type=F32).astype(BF)
        k0, k1 = PAIRS[i]
        close = k0 in NEAR
        k = k0 + c * (k1 - k0)
        there = lax.rem(NZ - k, NZ) if close else k
        for col in range(2):
            rows = done[:, col * HALF : (col + 1) * HALF].reshape(4, 4, CAP, HALF)
            pieces = [rows[j] if col == 0 else rows[:, j] for j in range(4)]
            for j in range(4):
                if j or close:
                    ysend[i, h, col, j] = pieces[j]
            for j in (1, 3, 2, 0) if close else (1, 3, 2):
                device = far(col, j, k if close else 0, h)
                remote(
                    ysend.at[i, h, col, j], r1buf.at[there, col, (-j) % 4], sent,
                    r1_recv.at[there, col], device,
                )
            if not close:

                @pl.when(c == h)
                def _():
                    r1buf[there, col, 0] = pieces[0]

                @pl.when(c != h)
                def _():
                    ysend[i, h, col, 0] = pieces[0]
                    remote(
                        ysend.at[i, h, col, 0], r1buf.at[there, col, 0], sent, r1_recv.at[there, col], partner
                    )

    def to_line(k, col, sums):
        pacc[k, col] = sums[:BLK]
        for j in range(1, 4):
            r2send[k, col, j - 1] = sums[BLK * j : BLK * j + BLK].astype(BF)
        for j in (1, 3, 2):
            remote(
                r2send.at[k, col, j - 1], r2buf.at[k, col, (-j) % 4 - 1], sent,
                r2_recv.at[LINED[k], col], peer(col, j),
            )

    def u7(k, col):
        if k in NEAR:
            drain(ysend.at[0, 0, 0], r1_recv.at[k, col])
        else:

            @pl.when(c == OWNER[k])
            def _():
                drain(ysend.at[0, 0, 0, pl.ds(1, 3)], r1_recv.at[k, col])

            @pl.when(c != OWNER[k])
            def _():
                drain(ysend.at[0, 0, 0], r1_recv.at[k, col])

        rows = r1buf[k, col].reshape(256, HALF)
        sums = lax.dot_general(select(k, col, True), rows, (((0,), (0,)), ((), ())), preferred_element_type=F32)
        if k == 0 or k in NEAR:
            if once(("e", col)):
                eacc[col] = sums
            else:
                eacc[col] += sums
        else:
            to_line(k, col, sums)

    def e2(k, col):
        to_line(0, col, eacc[col])

    def r8(k, col):
        drain(r2buf.at[k, col], r2_recv.at[LINED[k], col])
        total = pacc[k, col]
        for j in range(3):
            total = total + r2buf[k, col, j].astype(F32)
        slot = (-k) % NZ
        r3send[k, col] = total.astype(BF)
        remote(r3send.at[k, col], r3buf.at[slot, col], sent, r3_recv, at(dz=k))

    steps = (mb, s2, s3, ga, db, u7, r8, e2, zb)
    for step, k, col in SEQ:
        pl.when(c < 2)(lambda step=step, k=k, col=col: steps[step](k, col))

    part = []
    for col in range(2):
        drain(r2buf.at[0, col], r2_recv.at[0, col])
        total = pacc[0, col]
        for j in range(3):
            total = total + r2buf[0, col, j].astype(F32)
        part.append(total)
    drain(r3buf.at[pl.ds(0, NFAR)], r3_recv)
    for col in range(2):
        total = part[col]
        for k in DISTANT:
            total = total + r3buf[k, col].astype(F32)
        out_ref[:, col * HALF : (col + 1) * HALF] = total.astype(BF)

    drain(wg, sent)
    drain(wd.at[0], sent)
    drain(lsend.at[:, pl.ds(1, 3)], sent)
    drain(msrc.at[pl.ds(0, NFAR)], sent)
    drain(pbuf.at[pl.ds(0, len(SINGLE)), :, 0], sent)
    drain(pbuf.at[pl.ds(0, len(BUNDLE))], sent)
    drain(pbuf.at[pl.ds(0, len(SINGLE) + 1), :, pl.ds(1, 3)], sent)
    units = 56 + len(NEAR)
    for _ in range(2):
        drain(wg.at[:, pl.ds(0, 16 * units)], sent)
    drain(r2send.at[pl.ds(0, NFAR + 1)], sent)
    drain(r3send.at[pl.ds(0, NFAR)], sent)


def shards(tokens, norm_gain, routing, route_logits, w_gate, w_up, w_down):
    vmem = pltpu.VMEM
    dma = pltpu.SemaphoreType.DMA
    return pl.pallas_call(
        kernel,
        name="routed_layer",
        out_shape=vmem((BLK, 2 * HALF), BF),
        in_specs=[pl.BlockSpec(memory_space=pl.ANY)] * 7,
        out_specs=pl.BlockSpec(memory_space=vmem),
        scratch_shapes=[
            vmem((BLK, 1024), BF),
            vmem((1, 1024), F32),
            vmem((4, BLK), jnp.int32),
            vmem((4, BLK), F32),
            vmem((2, 1024, 512), BF),
            vmem((2, 1024, 512), BF),
            vmem((2, 1024, 512), BF),
            vmem((2, 4, 2, 8, 128), BF),
            vmem((2, 4, 2, 8, 128), BF),
            vmem((NZ, 2, 8, 128), BF),
            vmem((NZ, 2, 8, 128), BF),
            vmem((NZ, 2, 4, BLK, HALF), BF),
            vmem((NZ, 2, 4, 4, CAP, HALF), BF),
            vmem((4, 2, 2, 4, 4, CAP, HALF), BF),
            vmem((4, 2, 256, 512), BF),
            vmem((4, 2, 2, 4, 4, CAP, HALF), BF),
            vmem((NZ, 2, 4, 4, CAP, HALF), BF),
            vmem((2, 128, HALF), F32),
            vmem((NZ, 2, BLK, HALF), F32),
            vmem((NZ, 2, 3, BLK, HALF), BF),
            vmem((NZ, 2, 3, BLK, HALF), BF),
            vmem((NZ, 2, BLK, HALF), BF),
            vmem((NZ, 2, BLK, HALF), BF),
            dma((4,)),
            dma((2,)),
            dma((2,)),
            dma,
            dma,
            dma((NFAR,)),
            dma((len(SINGLE) + 1,)),
            dma((len(BUNDLE), 2)),
            dma((len(SINGLE) + 1, 2)),
            dma((4, 2)),
            dma((NZ, 2)),
            dma((NFAR + 1, 2)),
            dma,
        ],
        compiler_params=pltpu.CompilerParams(
            collective_id=0, has_side_effects=True, vmem_limit_bytes=60 * 1024 * 1024
        ),
    )(tokens, norm_gain.reshape(1, -1), routing.T, route_logits.T, w_gate[0], w_up[0], w_down[0])


def solution(mesh):
    return jax.shard_map(
        shards,
        mesh=mesh,
        in_specs=(
            P("ep", None),
            P(),
            P("ep", None),
            P("ep", None),
            P("ep", None, "tp"),
            P("ep", None, "tp"),
            P("ep", None, "tp"),
        ),
        out_specs=P("ep", "tp"),
        check_vma=False,
    )
```

```python
import jax
import jax.numpy as jnp
from jax import lax
from jax.experimental import pallas as pl
from jax.experimental.pallas import tpu as pltpu
from jax.sharding import PartitionSpec as P

MESH = pl.DeviceIdType.MESH
NX, NY, NZ = 4, 4, 8
CAP = 16
BLK = 32
HALF = 256
EPS = 1e-05
BF = jnp.bfloat16
F32 = jnp.float32
PAIRS = ((1, 0), (7, 2), (6, 3), (5, 4))
NEAR = ()
DISTANT = tuple(k for k in (1, 7, 2, 6, 3, 5, 4) if k not in NEAR)
NFAR = len(DISTANT)
BUNDLE = (3, 5)
SINGLE = tuple(k for k in DISTANT if k not in BUNDLE)
FAR = {k: n for n, k in enumerate(DISTANT)}
LINED = {k: n for n, k in enumerate((0,) + DISTANT)}
ALONE = {k: n for n, k in enumerate((0,) + SINGLE)}
OWNER = {k: c for pair in PAIRS for c, k in enumerate(pair)}
PLACE = {k: i for i, pair in enumerate(PAIRS) for k in pair}
SEQ = (
    (1, 1, 1), (1, 1, 0), (0, 0, 0), (8, 0, 1), (1, 7, 1), (1, 7, 0), (1, 6, 1), (2, 0, 1),
    (1, 2, 1), (1, 6, 0), (2, 0, 0), (1, 2, 0), (2, 7, 0), (2, 7, 1), (1, 4, 1), (2, 1, 0),
    (1, 4, 0), (8, 0, 0), (2, 6, 0), (2, 1, 1), (2, 2, 0), (2, 2, 1), (2, 6, 1), (2, 5, 1),
    (2, 4, 1), (2, 4, 0), (3, 0, 0), (2, 5, 0), (2, 3, 1), (2, 3, 0), (3, 0, 1), (3, 1, 0),
    (4, 0, 0), (3, 1, 1), (4, 1, 1), (4, 1, 0), (3, 3, 0), (3, 3, 1), (4, 3, 0), (3, 2, 0),
    (3, 2, 1), (4, 2, 0), (4, 3, 1), (4, 2, 1), (5, 4, 0), (5, 2, 1), (5, 5, 1), (5, 5, 0),
    (5, 3, 0), (5, 6, 0), (5, 4, 1), (5, 3, 1), (4, 0, 1), (5, 2, 0), (6, 4, 0), (6, 2, 1),
    (5, 6, 1), (6, 5, 0), (5, 1, 0), (5, 7, 1), (5, 7, 0), (5, 1, 1), (6, 5, 1), (6, 4, 1),
    (6, 3, 0), (5, 0, 0), (7, 0, 0), (6, 6, 0), (6, 3, 1), (6, 6, 1), (6, 2, 0), (5, 0, 1),
    (7, 0, 1), (6, 7, 1), (6, 1, 0), (6, 7, 0), (6, 1, 1),
)


def iota(shape, dim):
    return lax.broadcasted_iota(jnp.int32, shape, dim)


def kernel(
    tok_hbm, gain_hbm, ids_hbm, log_hbm, wg_hbm, wu_hbm, wd_hbm, out_ref,
    tok, gain, ids, logits, wg, wu, wd,
    lsend, lmeta, msrc, mtab, pbuf, sbuf, xbuf, hid, ysend, r1buf, eacc, pacc, r2send, r2buf, r3send, r3buf,
    in_sem, w_sem, w_recv, sent, l_recv, m_recv, z_recv, b_recv, s2_recv, x_recv, r1_recv, r2_recv, r3_recv,
):
    ep = lax.axis_index("ep")
    c = lax.axis_index("tp")
    x = lax.rem(ep, NX)
    y = lax.rem(ep // NX, NY)
    z = ep // (NX * NY)

    def at(dx=0, dy=0, dz=0, core=None):
        px = lax.rem(x + dx, NX)
        py = lax.rem(y + dy, NY)
        pz = lax.rem(z + dz, NZ)
        return ((pz * NY + py) * NX + px, c if core is None else core)

    partner = (ep, 1 - c)

    def peer(col, j):
        return at(dy=j) if col == 0 else at(dx=j)

    def far(col, j, dz, core):
        return at(dx=j, dz=dz, core=core) if col == 0 else at(dy=j, dz=dz, core=core)

    def remote(src, dst, send, recv, device):
        pltpu.make_async_remote_copy(
            src_ref=src, dst_ref=dst, send_sem=send, recv_sem=recv, device_id=device, device_id_type=MESH
        ).start()

    def drain(ref, sem):
        pltpu.make_async_copy(ref, ref, sem).wait()

    small = [
        pltpu.make_async_copy(tok_hbm, tok, in_sem.at[0]),
        pltpu.make_async_copy(gain_hbm, gain, in_sem.at[1]),
        pltpu.make_async_copy(ids_hbm, ids, in_sem.at[2]),
        pltpu.make_async_copy(log_hbm, logits, in_sem.at[3]),
    ]
    for copy in small:
        copy.start()

    barrier = pltpu.get_barrier_semaphore()
    both = (0, 1)
    friends = [partner]
    friends += [at(dy=j, core=o) for j in range(1, NY) for o in both]
    friends += [at(dx=j, core=o) for j in range(1, NX) for o in both]
    for k in NEAR:
        friends += [at(dz=k, core=o) for o in both]
        friends += [at(dy=j, dz=k, core=o) for j in range(1, NY) for o in both]
        friends += [at(dx=j, dz=k, core=o) for j in range(1, NX) for o in both]
    friends += [at(dz=k) for k in DISTANT]
    for friend in friends:
        pl.semaphore_signal(barrier, inc=1, device_id=friend, device_id_type=MESH)

    for copy in small:
        copy.wait()
    weights = ((wg_hbm, wg, 0), (wu_hbm, wu, 0), (wd_hbm, wd, 1))
    for src, dst, n in weights:
        pltpu.make_async_copy(src, dst.at[c], w_sem.at[n]).start()

    full = tok[...].astype(F32)
    scale = lax.rsqrt(jnp.mean(full * full, axis=-1, keepdims=True) + EPS)
    mine = pl.ds(pl.multiple_of(c * 512, 512), 512)
    normed = (tok[:, mine].astype(F32) * scale * gain[:, mine]).astype(BF)
    for col in range(2):
        pbuf[0, col, 0] = normed[:, col * HALF : (col + 1) * HALF]

    spread = (lax.rem(iota((BLK, 128), 1), BLK) == iota((BLK, 128), 0)).astype(BF)
    raw = logits[...]
    shifted = jnp.exp(raw - jnp.max(raw, axis=0, keepdims=True))
    probs = shifted / jnp.sum(shifted, axis=0, keepdims=True)
    ids_l = jnp.dot(ids[...].astype(F32).astype(BF), spread, preferred_element_type=F32)
    probs_l = jnp.dot(probs.astype(BF), spread, preferred_element_type=F32)
    row = iota((128, 128), 0)
    lane = iota((128, 128), 1)
    plane = lax.rem(z + lax.rem(row // 8, 2) * 4 + lane // BLK, NZ)
    group = lax.rem(row // 16, 4)
    near = lax.rem(row, 4)
    route_b = row < 64
    ex = lax.rem(x + jnp.where(route_b, near, group), NX)
    ey = lax.rem(y + jnp.where(route_b, group, near), NY)
    expert = (plane * 16 + ey * NX + ex).astype(F32)
    named = jnp.zeros((128, 128), F32)
    weight = jnp.zeros((128, 128), F32)
    for q in range(4):
        hit = expert == ids_l[q : q + 1, :]
        named = jnp.where(hit, 1.0, named)
        weight = jnp.where(hit, probs_l[q : q + 1, :], weight)
    before = ((row // BLK == lane // BLK) & (row < lane)).astype(BF)
    place = jnp.dot(named.astype(BF), before, preferred_element_type=F32)
    place = jnp.where(named > 0, place, -128.0)
    meta = jnp.where(lax.rem(row, 8) < 4, place, weight).astype(BF)
    for col in range(2):
        for g in range(4):
            for hi in range(2):
                start = col * 64 + g * 16 + hi * 8
                tile = meta[start : start + 8, :]
                if g:
                    lsend[col, g, hi] = tile
                else:
                    lmeta[col, 0, hi] = tile

    pl.semaphore_wait(barrier, len(friends))

    for col in range(2):
        for j in (2, 1, 3):
            remote(lsend.at[col, j], lmeta.at[col, (-j) % 4], sent, l_recv, peer(col, j))
            remote(pbuf.at[0, col, 0], pbuf.at[0, col, (-j) % 4], sent, s2_recv.at[0, col], peer(col, j))
    for k in SINGLE:
        slot = (-k) % NZ
        remote(pbuf.at[0, :, 0], pbuf.at[slot, :, 0], sent, z_recv.at[ALONE[slot]], at(dz=k))
    for src, dst, n in weights:
        remote(src, dst.at[c], sent, w_recv.at[n], partner)

    seen = set()

    def once(key):
        if key in seen:
            return False
        seen.add(key)
        return True

    def mb(k, col):
        lanes = iota((8, 128), 1) // BLK
        base = jnp.where(iota((8, 128), 0) < 4, lanes * CAP, 0).astype(F32)
        drain(lsend.at[:, pl.ds(1, 3)], l_recv)
        for col in range(2):
            for hi in range(2):
                t = [lmeta[col, s, hi].astype(F32) for s in range(4)]
                for lo in range(4):
                    turned = [t[s] if s == lo else pltpu.roll(t[s], BLK * ((s - lo) % 4), 1) for s in range(4)]
                    m = jnp.where(
                        lanes < 2, jnp.where(lanes == 0, turned[0], turned[1]), jnp.where(lanes == 2, turned[2], turned[3])
                    )
                    msrc[hi * 4 + lo, col] = (m + base).astype(BF)
        for k in DISTANT:
            slot = (-k) % NZ
            remote(msrc.at[k], mtab.at[slot], sent, m_recv.at[FAR[slot]], at(dz=k))

    def s2(k, col):
        if once(("z", k)):
            drain(pbuf.at[k, :, 0], z_recv.at[ALONE[k]])
        for j in (2, 1, 3):
            remote(pbuf.at[k, col, 0], pbuf.at[k, col, (-j) % 4], sent, s2_recv.at[ALONE[k], col], peer(col, j))

    def table(k, col):
        if k == 0 or k in NEAR:
            return msrc[k, col].astype(F32)
        return mtab[k, col].astype(F32)

    def select(k, col, weighted):
        m = table(k, col)
        sixty = iota((64, 128), 0).astype(F32)
        parts = []
        for j in range(4):
            value = m[4 + j : 5 + j, :] if weighted else 1.0
            parts.append(jnp.where(sixty == m[j : j + 1, :], value, 0.0).astype(BF))
        return jnp.concatenate(parts, axis=0)

    def lined(k, col):
        if once(("s2", k, col)):
            if k in BUNDLE:
                drain(pbuf.at[k, col], b_recv.at[BUNDLE.index(k), col])
            else:
                drain(pbuf.at[k, col, pl.ds(1, 3)], s2_recv.at[ALONE[k], col])

    def zb(k, col):
        lined(0, col)
        for k in BUNDLE:
            slot = (-k) % NZ
            remote(pbuf.at[0, col], pbuf.at[slot, col], sent, b_recv.at[BUNDLE.index(slot), col], at(dz=k))

    def s3(k, col):
        source = 0 if k in NEAR else k
        lined(source, col)
        if k in DISTANT and once(("m", k)):
            drain(mtab.at[k], m_recv.at[FAR[k]])
        rows = pbuf[source, col].reshape(128, HALF)
        packed = jnp.dot(select(k, col, False), rows, preferred_element_type=F32).astype(BF)
        there = (-k) % NZ if k in NEAR else k
        i, core = PLACE[there], OWNER[there]

        def target(slot):
            return xbuf.at[i, c, 0, slot] if col == 0 else xbuf.at[i, c, 1, :, slot]

        pieces = [packed[64 * j : 64 * j + 64].reshape(4, CAP, HALF) for j in range(4)]
        for j in range(4):
            if j or k in NEAR:
                sbuf[k, col, j] = pieces[j]
        for j in (1, 3, 2, 0) if k in NEAR else (2, 1, 3):
            device = far(col, j, k if k in NEAR else 0, core)
            remote(sbuf.at[k, col, j], target((-j) % 4), sent, x_recv.at[i, c], device)
        if k not in NEAR:

            @pl.when(c == core)
            def _():
                if col == 0:
                    xbuf[i, c, 0, 0] = pieces[0]
                else:
                    xbuf[i, c, 1, :, 0] = pieces[0]

            @pl.when(c != core)
            def _():
                sbuf[k, col, 0] = pieces[0]
                remote(sbuf.at[k, col, 0], target(0), sent, x_recv.at[i, c], partner)

    def ga(i, h):
        if once(("x", i)):
            drain(sbuf.at[0] if PAIRS[i][0] in NEAR else sbuf.at[0, :, pl.ds(1, 3)], x_recv.at[i, c])
            drain(sbuf.at[0], x_recv.at[i, 1 - c])
        if once("w"):
            drain(wg, w_sem.at[0])
            drain(wg, w_recv.at[0])
        rows = jnp.concatenate([xbuf[i, s, col].reshape(256, HALF) for s in range(2) for col in range(2)], axis=1)
        gate = jnp.minimum(jnp.dot(rows, wg[h], preferred_element_type=F32), 7.0)
        lin = jnp.clip(jnp.dot(rows, wu[h], preferred_element_type=F32), -7.0, 7.0)
        sig = 0.5 * jnp.tanh(0.851 * gate) + 0.5
        hid[i, h] = (gate * sig * (lin + 1.0)).astype(BF)

    def db(i, h):
        if once("d"):
            drain(wd.at[0], w_sem.at[1])
            drain(wd.at[0], w_recv.at[1])
        hidden = jnp.concatenate([hid[i, 0], hid[i, 1]], axis=1)
        done = jnp.dot(hidden, wd[h], preferred_element_type=F32).astype(BF)
        k0, k1 = PAIRS[i]
        close = k0 in NEAR
        k = k0 + c * (k1 - k0)
        there = lax.rem(NZ - k, NZ) if close else k
        for col in range(2):
            rows = done[:, col * HALF : (col + 1) * HALF].reshape(4, 4, CAP, HALF)
            pieces = [rows[j] if col == 0 else rows[:, j] for j in range(4)]
            for j in range(4):
                if j or close:
                    ysend[i, h, col, j] = pieces[j]
            for j in (1, 3, 2, 0) if close else (2, 1, 3):
                device = far(col, j, k if close else 0, h)
                remote(
                    ysend.at[i, h, col, j], r1buf.at[there, col, (-j) % 4], sent,
                    r1_recv.at[there, col], device,
                )
            if not close:

                @pl.when(c == h)
                def _():
                    r1buf[there, col, 0] = pieces[0]

                @pl.when(c != h)
                def _():
                    ysend[i, h, col, 0] = pieces[0]
                    remote(
                        ysend.at[i, h, col, 0], r1buf.at[there, col, 0], sent, r1_recv.at[there, col], partner
                    )

    def to_line(k, col, sums):
        pacc[k, col] = sums[:BLK]
        for j in range(1, 4):
            r2send[k, col, j - 1] = sums[BLK * j : BLK * j + BLK].astype(BF)
        for j in (2, 1, 3):
            remote(
                r2send.at[k, col, j - 1], r2buf.at[k, col, (-j) % 4 - 1], sent,
                r2_recv.at[LINED[k], col], peer(col, j),
            )

    def u7(k, col):
        if k in NEAR:
            drain(ysend.at[0, 0, 0], r1_recv.at[k, col])
        else:

            @pl.when(c == OWNER[k])
            def _():
                drain(ysend.at[0, 0, 0, pl.ds(1, 3)], r1_recv.at[k, col])

            @pl.when(c != OWNER[k])
            def _():
                drain(ysend.at[0, 0, 0], r1_recv.at[k, col])

        rows = r1buf[k, col].reshape(256, HALF)
        sums = lax.dot_general(select(k, col, True), rows, (((0,), (0,)), ((), ())), preferred_element_type=F32)
        if k == 0 or k in NEAR:
            if once(("e", col)):
                eacc[col] = sums
            else:
                eacc[col] += sums
        else:
            to_line(k, col, sums)

    def e2(k, col):
        to_line(0, col, eacc[col])

    def r8(k, col):
        drain(r2buf.at[k, col], r2_recv.at[LINED[k], col])
        total = pacc[k, col]
        for j in range(3):
            total = total + r2buf[k, col, j].astype(F32)
        slot = (-k) % NZ
        r3send[k, col] = total.astype(BF)
        remote(r3send.at[k, col], r3buf.at[slot, col], sent, r3_recv, at(dz=k))

    steps = (mb, s2, s3, ga, db, u7, r8, e2, zb)
    for step, k, col in SEQ:
        pl.when(c < 2)(lambda step=step, k=k, col=col: steps[step](k, col))

    part = []
    for col in range(2):
        drain(r2buf.at[0, col], r2_recv.at[0, col])
        total = pacc[0, col]
        for j in range(3):
            total = total + r2buf[0, col, j].astype(F32)
        part.append(total)
    drain(r3buf.at[pl.ds(0, NFAR)], r3_recv)
    for col in range(2):
        total = part[col]
        for k in DISTANT:
            total = total + r3buf[k, col].astype(F32)
        out_ref[:, col * HALF : (col + 1) * HALF] = total.astype(BF)

    drain(wg, sent)
    drain(wd.at[0], sent)
    drain(lsend.at[:, pl.ds(1, 3)], sent)
    drain(msrc.at[pl.ds(0, NFAR)], sent)
    drain(pbuf.at[pl.ds(0, len(SINGLE)), :, 0], sent)
    drain(pbuf.at[pl.ds(0, len(BUNDLE))], sent)
    drain(pbuf.at[pl.ds(0, len(SINGLE) + 1), :, pl.ds(1, 3)], sent)
    units = 56 + len(NEAR)
    for _ in range(2):
        drain(wg.at[:, pl.ds(0, 16 * units)], sent)
    drain(r2send.at[pl.ds(0, NFAR + 1)], sent)
    drain(r3send.at[pl.ds(0, NFAR)], sent)


def shards(tokens, norm_gain, routing, route_logits, w_gate, w_up, w_down):
    vmem = pltpu.VMEM
    dma = pltpu.SemaphoreType.DMA
    return pl.pallas_call(
        kernel,
        name="routed_layer",
        out_shape=vmem((BLK, 2 * HALF), BF),
        in_specs=[pl.BlockSpec(memory_space=pl.ANY)] * 7,
        out_specs=pl.BlockSpec(memory_space=vmem),
        scratch_shapes=[
            vmem((BLK, 1024), BF),
            vmem((1, 1024), F32),
            vmem((4, BLK), jnp.int32),
            vmem((4, BLK), F32),
            vmem((2, 1024, 512), BF),
            vmem((2, 1024, 512), BF),
            vmem((2, 1024, 512), BF),
            vmem((2, 4, 2, 8, 128), BF),
            vmem((2, 4, 2, 8, 128), BF),
            vmem((NZ, 2, 8, 128), BF),
            vmem((NZ, 2, 8, 128), BF),
            vmem((NZ, 2, 4, BLK, HALF), BF),
            vmem((NZ, 2, 4, 4, CAP, HALF), BF),
            vmem((4, 2, 2, 4, 4, CAP, HALF), BF),
            vmem((4, 2, 256, 512), BF),
            vmem((4, 2, 2, 4, 4, CAP, HALF), BF),
            vmem((NZ, 2, 4, 4, CAP, HALF), BF),
            vmem((2, 128, HALF), F32),
            vmem((NZ, 2, BLK, HALF), F32),
            vmem((NZ, 2, 3, BLK, HALF), BF),
            vmem((NZ, 2, 3, BLK, HALF), BF),
            vmem((NZ, 2, BLK, HALF), BF),
            vmem((NZ, 2, BLK, HALF), BF),
            dma((4,)),
            dma((2,)),
            dma((2,)),
            dma,
            dma,
            dma((NFAR,)),
            dma((len(SINGLE) + 1,)),
            dma((len(BUNDLE), 2)),
            dma((len(SINGLE) + 1, 2)),
            dma((4, 2)),
            dma((NZ, 2)),
            dma((NFAR + 1, 2)),
            dma,
        ],
        compiler_params=pltpu.CompilerParams(
            collective_id=0, has_side_effects=True, vmem_limit_bytes=60 * 1024 * 1024
        ),
    )(tokens, norm_gain.reshape(1, -1), routing.T, route_logits.T, w_gate[0], w_up[0], w_down[0])


def solution(mesh):
    return jax.shard_map(
        shards,
        mesh=mesh,
        in_specs=(
            P("ep", None),
            P(),
            P("ep", None),
            P("ep", None),
            P("ep", None, "tp"),
            P("ep", None, "tp"),
            P("ep", None, "tp"),
        ),
        out_specs=P("ep", "tp"),
        check_vma=False,
    )
```

```python
import jax
import jax.numpy as jnp
from jax import lax
from jax.experimental import pallas as pl
from jax.experimental.pallas import tpu as pltpu
from jax.sharding import PartitionSpec as P

MESH = pl.DeviceIdType.MESH
NX, NY, NZ = 4, 4, 8
CAP = 16
BLK = 32
HALF = 256
EPS = 1e-05
BF = jnp.bfloat16
F32 = jnp.float32
PAIRS = ((1, 0), (7, 2), (6, 3), (5, 4))
NEAR = ()
DISTANT = tuple(k for k in (1, 7, 2, 6, 3, 5, 4) if k not in NEAR)
NFAR = len(DISTANT)
BUNDLE = (3, 5)
SINGLE = tuple(k for k in DISTANT if k not in BUNDLE)
FAR = {k: n for n, k in enumerate(DISTANT)}
LINED = {k: n for n, k in enumerate((0,) + DISTANT)}
ALONE = {k: n for n, k in enumerate((0,) + SINGLE)}
OWNER = {k: c for pair in PAIRS for c, k in enumerate(pair)}
PLACE = {k: i for i, pair in enumerate(PAIRS) for k in pair}
SEQ = (
    (1, 7, 1), (1, 1, 0), (0, 0, 0), (1, 1, 1), (1, 7, 0), (8, 0, 1), (8, 0, 0), (2, 0, 1),
    (2, 0, 0), (1, 2, 0), (1, 2, 1), (1, 6, 0), (1, 6, 1), (2, 1, 0), (2, 1, 1), (1, 4, 1),
    (1, 4, 0), (2, 2, 1), (2, 7, 0), (2, 7, 1), (2, 2, 0), (2, 4, 0), (2, 5, 1), (2, 6, 0),
    (2, 6, 1), (2, 4, 1), (2, 3, 1), (3, 0, 0), (2, 5, 0), (3, 0, 1), (2, 3, 0), (3, 1, 0),
    (4, 0, 0), (3, 1, 1), (4, 1, 0), (4, 1, 1), (3, 3, 0), (3, 3, 1), (4, 3, 0), (3, 2, 0),
    (3, 2, 1), (4, 2, 0), (4, 3, 1), (4, 2, 1), (5, 4, 0), (5, 4, 1), (5, 5, 1), (5, 2, 1),
    (5, 3, 0), (5, 5, 0), (5, 6, 0), (5, 3, 1), (4, 0, 1), (6, 4, 1), (5, 2, 0), (5, 6, 1),
    (5, 7, 1), (6, 5, 1), (6, 3, 0), (6, 4, 0), (6, 2, 1), (5, 1, 0), (6, 5, 0), (5, 1, 1),
    (5, 7, 0), (6, 3, 1), (6, 2, 0), (6, 6, 0), (5, 0, 0), (7, 0, 0), (5, 0, 1), (7, 0, 1),
    (6, 6, 1), (6, 7, 1), (6, 1, 0), (6, 1, 1), (6, 7, 0),
)


def iota(shape, dim):
    return lax.broadcasted_iota(jnp.int32, shape, dim)


def kernel(
    tok_hbm, gain_hbm, ids_hbm, log_hbm, wg_hbm, wu_hbm, wd_hbm, out_ref,
    tok, gain, ids, logits, wg, wu, wd,
    lsend, lmeta, msrc, mtab, pbuf, sbuf, xbuf, hid, ysend, r1buf, eacc, pacc, r2send, r2buf, r3send, r3buf,
    in_sem, w_sem, w_recv, sent, l_recv, m_recv, z_recv, b_recv, s2_recv, x_recv, r1_recv, r2_recv, r3_recv,
):
    ep = lax.axis_index("ep")
    c = lax.axis_index("tp")
    x = lax.rem(ep, NX)
    y = lax.rem(ep // NX, NY)
    z = ep // (NX * NY)

    def at(dx=0, dy=0, dz=0, core=None):
        px = lax.rem(x + dx, NX)
        py = lax.rem(y + dy, NY)
        pz = lax.rem(z + dz, NZ)
        return ((pz * NY + py) * NX + px, c if core is None else core)

    partner = (ep, 1 - c)

    def peer(col, j):
        return at(dy=j) if col == 0 else at(dx=j)

    def far(col, j, dz, core):
        return at(dx=j, dz=dz, core=core) if col == 0 else at(dy=j, dz=dz, core=core)

    def remote(src, dst, send, recv, device):
        pltpu.make_async_remote_copy(
            src_ref=src, dst_ref=dst, send_sem=send, recv_sem=recv, device_id=device, device_id_type=MESH
        ).start()

    def drain(ref, sem):
        pltpu.make_async_copy(ref, ref, sem).wait()

    small = [
        pltpu.make_async_copy(tok_hbm, tok, in_sem.at[0]),
        pltpu.make_async_copy(gain_hbm, gain, in_sem.at[1]),
        pltpu.make_async_copy(ids_hbm, ids, in_sem.at[2]),
        pltpu.make_async_copy(log_hbm, logits, in_sem.at[3]),
    ]
    for copy in small:
        copy.start()

    barrier = pltpu.get_barrier_semaphore()
    both = (0, 1)
    friends = [partner]
    friends += [at(dy=j, core=o) for j in range(1, NY) for o in both]
    friends += [at(dx=j, core=o) for j in range(1, NX) for o in both]
    for k in NEAR:
        friends += [at(dz=k, core=o) for o in both]
        friends += [at(dy=j, dz=k, core=o) for j in range(1, NY) for o in both]
        friends += [at(dx=j, dz=k, core=o) for j in range(1, NX) for o in both]
    friends += [at(dz=k) for k in DISTANT]
    for friend in friends:
        pl.semaphore_signal(barrier, inc=1, device_id=friend, device_id_type=MESH)

    for copy in small:
        copy.wait()
    weights = ((wg_hbm, wg, 0), (wu_hbm, wu, 0), (wd_hbm, wd, 1))
    for src, dst, n in weights:
        pltpu.make_async_copy(src, dst.at[c], w_sem.at[n]).start()

    full = tok[...].astype(F32)
    scale = lax.rsqrt(jnp.mean(full * full, axis=-1, keepdims=True) + EPS)
    mine = pl.ds(pl.multiple_of(c * 512, 512), 512)
    normed = (tok[:, mine].astype(F32) * scale * gain[:, mine]).astype(BF)
    for col in range(2):
        pbuf[0, col, 0] = normed[:, col * HALF : (col + 1) * HALF]

    spread = (lax.rem(iota((BLK, 128), 1), BLK) == iota((BLK, 128), 0)).astype(BF)
    raw = logits[...]
    shifted = jnp.exp(raw - jnp.max(raw, axis=0, keepdims=True))
    probs = shifted / jnp.sum(shifted, axis=0, keepdims=True)
    ids_l = jnp.dot(ids[...].astype(F32).astype(BF), spread, preferred_element_type=F32)
    probs_l = jnp.dot(probs.astype(BF), spread, preferred_element_type=F32)
    row = iota((128, 128), 0)
    lane = iota((128, 128), 1)
    plane = lax.rem(z + lax.rem(row // 8, 2) * 4 + lane // BLK, NZ)
    group = lax.rem(row // 16, 4)
    near = lax.rem(row, 4)
    route_b = row < 64
    ex = lax.rem(x + jnp.where(route_b, near, group), NX)
    ey = lax.rem(y + jnp.where(route_b, group, near), NY)
    expert = (plane * 16 + ey * NX + ex).astype(F32)
    named = jnp.zeros((128, 128), F32)
    weight = jnp.zeros((128, 128), F32)
    for q in range(4):
        hit = expert == ids_l[q : q + 1, :]
        named = jnp.where(hit, 1.0, named)
        weight = jnp.where(hit, probs_l[q : q + 1, :], weight)
    before = ((row // BLK == lane // BLK) & (row < lane)).astype(BF)
    place = jnp.dot(named.astype(BF), before, preferred_element_type=F32)
    place = jnp.where(named > 0, place, -128.0)
    meta = jnp.where(lax.rem(row, 8) < 4, place, weight).astype(BF)
    for col in range(2):
        for g in range(4):
            for hi in range(2):
                start = col * 64 + g * 16 + hi * 8
                tile = meta[start : start + 8, :]
                if g:
                    lsend[col, g, hi] = tile
                else:
                    lmeta[col, 0, hi] = tile

    pl.semaphore_wait(barrier, len(friends))

    for col in range(2):
        for j in (2, 1, 3):
            remote(lsend.at[col, j], lmeta.at[col, (-j) % 4], sent, l_recv, peer(col, j))
            remote(pbuf.at[0, col, 0], pbuf.at[0, col, (-j) % 4], sent, s2_recv.at[0, col], peer(col, j))
    for k in SINGLE:
        slot = (-k) % NZ
        remote(pbuf.at[0, :, 0], pbuf.at[slot, :, 0], sent, z_recv.at[ALONE[slot]], at(dz=k))
    for src, dst, n in weights:
        remote(src, dst.at[c], sent, w_recv.at[n], partner)

    seen = set()

    def once(key):
        if key in seen:
            return False
        seen.add(key)
        return True

    def mb(k, col):
        lanes = iota((8, 128), 1) // BLK
        base = jnp.where(iota((8, 128), 0) < 4, lanes * CAP, 0).astype(F32)
        drain(lsend.at[:, pl.ds(1, 3)], l_recv)
        for col in range(2):
            for hi in range(2):
                t = [lmeta[col, s, hi].astype(F32) for s in range(4)]
                for lo in range(4):
                    turned = [t[s] if s == lo else pltpu.roll(t[s], BLK * ((s - lo) % 4), 1) for s in range(4)]
                    m = jnp.where(
                        lanes < 2, jnp.where(lanes == 0, turned[0], turned[1]), jnp.where(lanes == 2, turned[2], turned[3])
                    )
                    msrc[hi * 4 + lo, col] = (m + base).astype(BF)
        for k in DISTANT:
            slot = (-k) % NZ
            remote(msrc.at[k], mtab.at[slot], sent, m_recv.at[FAR[slot]], at(dz=k))

    def s2(k, col):
        if once(("z", k)):
            drain(pbuf.at[k, :, 0], z_recv.at[ALONE[k]])
        for j in (2, 1, 3):
            remote(pbuf.at[k, col, 0], pbuf.at[k, col, (-j) % 4], sent, s2_recv.at[ALONE[k], col], peer(col, j))

    def table(k, col):
        if k == 0 or k in NEAR:
            return msrc[k, col].astype(F32)
        return mtab[k, col].astype(F32)

    def select(k, col, weighted):
        m = table(k, col)
        sixty = iota((64, 128), 0).astype(F32)
        parts = []
        for j in range(4):
            value = m[4 + j : 5 + j, :] if weighted else 1.0
            parts.append(jnp.where(sixty == m[j : j + 1, :], value, 0.0).astype(BF))
        return jnp.concatenate(parts, axis=0)

    def lined(k, col):
        if once(("s2", k, col)):
            if k in BUNDLE:
                drain(pbuf.at[k, col], b_recv.at[BUNDLE.index(k), col])
            else:
                drain(pbuf.at[k, col, pl.ds(1, 3)], s2_recv.at[ALONE[k], col])

    def zb(k, col):
        lined(0, col)
        for k in BUNDLE:
            slot = (-k) % NZ
            remote(pbuf.at[0, col], pbuf.at[slot, col], sent, b_recv.at[BUNDLE.index(slot), col], at(dz=k))

    def s3(k, col):
        source = 0 if k in NEAR else k
        lined(source, col)
        if k in DISTANT and once(("m", k)):
            drain(mtab.at[k], m_recv.at[FAR[k]])
        rows = pbuf[source, col].reshape(128, HALF)
        packed = jnp.dot(select(k, col, False), rows, preferred_element_type=F32).astype(BF)
        there = (-k) % NZ if k in NEAR else k
        i, core = PLACE[there], OWNER[there]

        def target(slot):
            return xbuf.at[i, c, 0, slot] if col == 0 else xbuf.at[i, c, 1, :, slot]

        pieces = [packed[64 * j : 64 * j + 64].reshape(4, CAP, HALF) for j in range(4)]
        for j in range(4):
            if j or k in NEAR:
                sbuf[k, col, j] = pieces[j]
        for j in (1, 3, 2, 0) if k in NEAR else (2, 1, 3):
            device = far(col, j, k if k in NEAR else 0, core)
            remote(sbuf.at[k, col, j], target((-j) % 4), sent, x_recv.at[i, c], device)
        if k not in NEAR:

            @pl.when(c == core)
            def _():
                if col == 0:
                    xbuf[i, c, 0, 0] = pieces[0]
                else:
                    xbuf[i, c, 1, :, 0] = pieces[0]

            @pl.when(c != core)
            def _():
                sbuf[k, col, 0] = pieces[0]
                remote(sbuf.at[k, col, 0], target(0), sent, x_recv.at[i, c], partner)

    def ga(i, h):
        if once(("x", i)):
            drain(sbuf.at[0] if PAIRS[i][0] in NEAR else sbuf.at[0, :, pl.ds(1, 3)], x_recv.at[i, c])
            drain(sbuf.at[0], x_recv.at[i, 1 - c])
        if once("w"):
            drain(wg, w_sem.at[0])
            drain(wg, w_recv.at[0])
        rows = jnp.concatenate([xbuf[i, s, col].reshape(256, HALF) for s in range(2) for col in range(2)], axis=1)
        gate = jnp.minimum(jnp.dot(rows, wg[h], preferred_element_type=F32), 7.0)
        lin = jnp.clip(jnp.dot(rows, wu[h], preferred_element_type=F32), -7.0, 7.0)
        sig = 0.5 * jnp.tanh(0.851 * gate) + 0.5
        hid[i, h] = (gate * sig * (lin + 1.0)).astype(BF)

    def db(i, h):
        if once("d"):
            drain(wd.at[0], w_sem.at[1])
            drain(wd.at[0], w_recv.at[1])
        hidden = jnp.concatenate([hid[i, 0], hid[i, 1]], axis=1)
        done = jnp.dot(hidden, wd[h], preferred_element_type=F32).astype(BF)
        k0, k1 = PAIRS[i]
        close = k0 in NEAR
        k = k0 + c * (k1 - k0)
        there = lax.rem(NZ - k, NZ) if close else k
        for col in range(2):
            rows = done[:, col * HALF : (col + 1) * HALF].reshape(4, 4, CAP, HALF)
            pieces = [rows[j] if col == 0 else rows[:, j] for j in range(4)]
            for j in range(4):
                if j or close:
                    ysend[i, h, col, j] = pieces[j]
            for j in (1, 3, 2, 0) if close else (2, 1, 3):
                device = far(col, j, k if close else 0, h)
                remote(
                    ysend.at[i, h, col, j], r1buf.at[there, col, (-j) % 4], sent,
                    r1_recv.at[there, col], device,
                )
            if not close:

                @pl.when(c == h)
                def _():
                    r1buf[there, col, 0] = pieces[0]

                @pl.when(c != h)
                def _():
                    ysend[i, h, col, 0] = pieces[0]
                    remote(
                        ysend.at[i, h, col, 0], r1buf.at[there, col, 0], sent, r1_recv.at[there, col], partner
                    )

    def to_line(k, col, sums):
        pacc[k, col] = sums[:BLK]
        for j in range(1, 4):
            r2send[k, col, j - 1] = sums[BLK * j : BLK * j + BLK].astype(BF)
        for j in (2, 1, 3):
            remote(
                r2send.at[k, col, j - 1], r2buf.at[k, col, (-j) % 4 - 1], sent,
                r2_recv.at[LINED[k], col], peer(col, j),
            )

    def u7(k, col):
        if k in NEAR:
            drain(ysend.at[0, 0, 0], r1_recv.at[k, col])
        else:

            @pl.when(c == OWNER[k])
            def _():
                drain(ysend.at[0, 0, 0, pl.ds(1, 3)], r1_recv.at[k, col])

            @pl.when(c != OWNER[k])
            def _():
                drain(ysend.at[0, 0, 0], r1_recv.at[k, col])

        rows = r1buf[k, col].reshape(256, HALF)
        sums = lax.dot_general(select(k, col, True), rows, (((0,), (0,)), ((), ())), preferred_element_type=F32)
        if k == 0 or k in NEAR:
            if once(("e", col)):
                eacc[col] = sums
            else:
                eacc[col] += sums
        else:
            to_line(k, col, sums)

    def e2(k, col):
        to_line(0, col, eacc[col])

    def r8(k, col):
        drain(r2buf.at[k, col], r2_recv.at[LINED[k], col])
        total = pacc[k, col]
        for j in range(3):
            total = total + r2buf[k, col, j].astype(F32)
        slot = (-k) % NZ
        r3send[k, col] = total.astype(BF)
        remote(r3send.at[k, col], r3buf.at[slot, col], sent, r3_recv, at(dz=k))

    steps = (mb, s2, s3, ga, db, u7, r8, e2, zb)
    for step, k, col in SEQ:
        pl.when(c < 2)(lambda step=step, k=k, col=col: steps[step](k, col))

    part = []
    for col in range(2):
        drain(r2buf.at[0, col], r2_recv.at[0, col])
        total = pacc[0, col]
        for j in range(3):
            total = total + r2buf[0, col, j].astype(F32)
        part.append(total)
    drain(r3buf.at[pl.ds(0, NFAR)], r3_recv)
    for col in range(2):
        total = part[col]
        for k in DISTANT:
            total = total + r3buf[k, col].astype(F32)
        out_ref[:, col * HALF : (col + 1) * HALF] = total.astype(BF)

    drain(wg, sent)
    drain(wd.at[0], sent)
    drain(lsend.at[:, pl.ds(1, 3)], sent)
    drain(msrc.at[pl.ds(0, NFAR)], sent)
    drain(pbuf.at[pl.ds(0, len(SINGLE)), :, 0], sent)
    drain(pbuf.at[pl.ds(0, len(BUNDLE))], sent)
    drain(pbuf.at[pl.ds(0, len(SINGLE) + 1), :, pl.ds(1, 3)], sent)
    units = 56 + len(NEAR)
    for _ in range(2):
        drain(wg.at[:, pl.ds(0, 16 * units)], sent)
    drain(r2send.at[pl.ds(0, NFAR + 1)], sent)
    drain(r3send.at[pl.ds(0, NFAR)], sent)


def shards(tokens, norm_gain, routing, route_logits, w_gate, w_up, w_down):
    vmem = pltpu.VMEM
    dma = pltpu.SemaphoreType.DMA
    return pl.pallas_call(
        kernel,
        name="routed_layer",
        out_shape=vmem((BLK, 2 * HALF), BF),
        in_specs=[pl.BlockSpec(memory_space=pl.ANY)] * 7,
        out_specs=pl.BlockSpec(memory_space=vmem),
        scratch_shapes=[
            vmem((BLK, 1024), BF),
            vmem((1, 1024), F32),
            vmem((4, BLK), jnp.int32),
            vmem((4, BLK), F32),
            vmem((2, 1024, 512), BF),
            vmem((2, 1024, 512), BF),
            vmem((2, 1024, 512), BF),
            vmem((2, 4, 2, 8, 128), BF),
            vmem((2, 4, 2, 8, 128), BF),
            vmem((NZ, 2, 8, 128), BF),
            vmem((NZ, 2, 8, 128), BF),
            vmem((NZ, 2, 4, BLK, HALF), BF),
            vmem((NZ, 2, 4, 4, CAP, HALF), BF),
            vmem((4, 2, 2, 4, 4, CAP, HALF), BF),
            vmem((4, 2, 256, 512), BF),
            vmem((4, 2, 2, 4, 4, CAP, HALF), BF),
            vmem((NZ, 2, 4, 4, CAP, HALF), BF),
            vmem((2, 128, HALF), F32),
            vmem((NZ, 2, BLK, HALF), F32),
            vmem((NZ, 2, 3, BLK, HALF), BF),
            vmem((NZ, 2, 3, BLK, HALF), BF),
            vmem((NZ, 2, BLK, HALF), BF),
            vmem((NZ, 2, BLK, HALF), BF),
            dma((4,)),
            dma((2,)),
            dma((2,)),
            dma,
            dma,
            dma((NFAR,)),
            dma((len(SINGLE) + 1,)),
            dma((len(BUNDLE), 2)),
            dma((len(SINGLE) + 1, 2)),
            dma((4, 2)),
            dma((NZ, 2)),
            dma((NFAR + 1, 2)),
            dma,
        ],
        compiler_params=pltpu.CompilerParams(
            collective_id=0, has_side_effects=True, vmem_limit_bytes=60 * 1024 * 1024
        ),
    )(tokens, norm_gain.reshape(1, -1), routing.T, route_logits.T, w_gate[0], w_up[0], w_down[0])


def solution(mesh):
    return jax.shard_map(
        shards,
        mesh=mesh,
        in_specs=(
            P("ep", None),
            P(),
            P("ep", None),
            P("ep", None),
            P("ep", None, "tp"),
            P("ep", None, "tp"),
            P("ep", None, "tp"),
        ),
        out_specs=P("ep", "tp"),
        check_vma=False,
    )
```

```python
import jax
import jax.numpy as jnp
from jax import lax
from jax.experimental import pallas as pl
from jax.experimental.pallas import tpu as pltpu
from jax.sharding import PartitionSpec as P

MESH = pl.DeviceIdType.MESH
NX, NY, NZ = 4, 4, 8
CAP = 16
BLK = 32
HALF = 256
EPS = 1e-05
BF = jnp.bfloat16
F32 = jnp.float32
PAIRS = ((1, 0), (7, 2), (6, 3), (5, 4))
NEAR = ()
DISTANT = tuple(k for k in (1, 7, 2, 6, 3, 5, 4) if k not in NEAR)
NFAR = len(DISTANT)
BUNDLE = (3, 5)
SINGLE = tuple(k for k in DISTANT if k not in BUNDLE)
FAR = {k: n for n, k in enumerate(DISTANT)}
LINED = {k: n for n, k in enumerate((0,) + DISTANT)}
ALONE = {k: n for n, k in enumerate((0,) + SINGLE)}
OWNER = {k: c for pair in PAIRS for c, k in enumerate(pair)}
PLACE = {k: i for i, pair in enumerate(PAIRS) for k in pair}
SEQ = (
    (1, 7, 1), (1, 1, 0), (0, 0, 0), (1, 1, 1), (1, 7, 0), (8, 0, 1), (8, 0, 0), (2, 0, 1),
    (2, 0, 0), (1, 2, 0), (1, 2, 1), (1, 6, 0), (1, 6, 1), (2, 1, 0), (2, 1, 1), (1, 4, 1),
    (1, 4, 0), (2, 2, 1), (2, 7, 0), (2, 7, 1), (2, 2, 0), (2, 4, 0), (2, 5, 1), (2, 6, 0),
    (2, 6, 1), (2, 4, 1), (2, 3, 1), (3, 0, 0), (2, 5, 0), (3, 0, 1), (2, 3, 0), (3, 1, 0),
    (4, 0, 0), (3, 1, 1), (4, 1, 0), (4, 1, 1), (3, 3, 0), (3, 3, 1), (4, 3, 0), (3, 2, 0),
    (3, 2, 1), (4, 2, 0), (4, 3, 1), (4, 2, 1), (5, 4, 0), (5, 4, 1), (5, 5, 1), (5, 2, 1),
    (5, 3, 0), (5, 5, 0), (5, 6, 0), (5, 3, 1), (4, 0, 1), (6, 4, 1), (5, 2, 0), (5, 6, 1),
    (5, 7, 1), (6, 5, 1), (6, 3, 0), (6, 4, 0), (6, 2, 1), (5, 1, 0), (6, 5, 0), (5, 1, 1),
    (5, 7, 0), (6, 3, 1), (6, 2, 0), (6, 6, 0), (5, 0, 0), (7, 0, 0), (5, 0, 1), (7, 0, 1),
    (6, 6, 1), (6, 7, 1), (6, 1, 0), (6, 1, 1), (6, 7, 0),
)


def iota(shape, dim):
    return lax.broadcasted_iota(jnp.int32, shape, dim)


def kernel(
    tok_hbm, gain_hbm, ids_hbm, log_hbm, wg_hbm, wu_hbm, wd_hbm, out_ref,
    tok, gain, ids, logits, wg, wu, wd,
    lsend, lmeta, msrc, mtab, pbuf, sbuf, xbuf, hid, ysend, r1buf, eacc, pacc, r2send, r2buf, r3send, r3buf,
    in_sem, w_sem, w_recv, sent, l_recv, m_recv, z_recv, b_recv, s2_recv, x_recv, r1_recv, r2_recv, r3_recv,
):
    ep = lax.axis_index("ep")
    c = lax.axis_index("tp")
    x = lax.rem(ep, NX)
    y = lax.rem(ep // NX, NY)
    z = ep // (NX * NY)

    def at(dx=0, dy=0, dz=0, core=None):
        px = lax.rem(x + dx, NX)
        py = lax.rem(y + dy, NY)
        pz = lax.rem(z + dz, NZ)
        return ((pz * NY + py) * NX + px, c if core is None else core)

    partner = (ep, 1 - c)

    def peer(col, j):
        return at(dy=j) if col == 0 else at(dx=j)

    def far(col, j, dz, core):
        return at(dx=j, dz=dz, core=core) if col == 0 else at(dy=j, dz=dz, core=core)

    def remote(src, dst, send, recv, device):
        pltpu.make_async_remote_copy(
            src_ref=src, dst_ref=dst, send_sem=send, recv_sem=recv, device_id=device, device_id_type=MESH
        ).start()

    def drain(ref, sem):
        pltpu.make_async_copy(ref, ref, sem).wait()

    small = [
        pltpu.make_async_copy(tok_hbm, tok, in_sem.at[0]),
        pltpu.make_async_copy(gain_hbm, gain, in_sem.at[1]),
        pltpu.make_async_copy(ids_hbm, ids, in_sem.at[2]),
        pltpu.make_async_copy(log_hbm, logits, in_sem.at[3]),
    ]
    for copy in small:
        copy.start()

    barrier = pltpu.get_barrier_semaphore()
    both = (0, 1)
    friends = [partner]
    friends += [at(dy=j, core=o) for j in range(1, NY) for o in both]
    friends += [at(dx=j, core=o) for j in range(1, NX) for o in both]
    for k in NEAR:
        friends += [at(dz=k, core=o) for o in both]
        friends += [at(dy=j, dz=k, core=o) for j in range(1, NY) for o in both]
        friends += [at(dx=j, dz=k, core=o) for j in range(1, NX) for o in both]
    friends += [at(dz=k) for k in DISTANT]
    for friend in friends:
        pl.semaphore_signal(barrier, inc=1, device_id=friend, device_id_type=MESH)

    for copy in small:
        copy.wait()
    weights = ((wg_hbm, wg, 0), (wu_hbm, wu, 0), (wd_hbm, wd, 1))
    for src, dst, n in weights:
        pltpu.make_async_copy(src, dst.at[c], w_sem.at[n]).start()

    full = tok[...].astype(F32)
    scale = lax.rsqrt(jnp.mean(full * full, axis=-1, keepdims=True) + EPS)
    mine = pl.ds(pl.multiple_of(c * 512, 512), 512)
    normed = (tok[:, mine].astype(F32) * scale * gain[:, mine]).astype(BF)
    for col in range(2):
        pbuf[0, col, 0] = normed[:, col * HALF : (col + 1) * HALF]

    spread = (lax.rem(iota((BLK, 128), 1), BLK) == iota((BLK, 128), 0)).astype(BF)
    raw = logits[...]
    shifted = jnp.exp(raw - jnp.max(raw, axis=0, keepdims=True))
    probs = shifted / jnp.sum(shifted, axis=0, keepdims=True)
    ids_l = jnp.dot(ids[...].astype(F32).astype(BF), spread, preferred_element_type=F32)
    probs_l = jnp.dot(probs.astype(BF), spread, preferred_element_type=F32)
    row = iota((128, 128), 0)
    lane = iota((128, 128), 1)
    plane = lax.rem(z + lax.rem(row // 8, 2) * 4 + lane // BLK, NZ)
    group = lax.rem(row // 16, 4)
    near = lax.rem(row, 4)
    route_b = row < 64
    ex = lax.rem(x + jnp.where(route_b, near, group), NX)
    ey = lax.rem(y + jnp.where(route_b, group, near), NY)
    expert = (plane * 16 + ey * NX + ex).astype(F32)
    named = jnp.zeros((128, 128), F32)
    weight = jnp.zeros((128, 128), F32)
    for q in range(4):
        hit = expert == ids_l[q : q + 1, :]
        named = jnp.where(hit, 1.0, named)
        weight = jnp.where(hit, probs_l[q : q + 1, :], weight)
    before = ((row // BLK == lane // BLK) & (row < lane)).astype(BF)
    place = jnp.dot(named.astype(BF), before, preferred_element_type=F32)
    place = jnp.where(named > 0, place, -128.0)
    meta = jnp.where(lax.rem(row, 8) < 4, place, weight).astype(BF)
    for col in range(2):
        for g in range(4):
            for hi in range(2):
                start = col * 64 + g * 16 + hi * 8
                tile = meta[start : start + 8, :]
                if g:
                    lsend[col, g, hi] = tile
                else:
                    lmeta[col, 0, hi] = tile

    pl.semaphore_wait(barrier, len(friends))

    for col in range(2):
        for j in (2, 1, 3):
            remote(lsend.at[col, j], lmeta.at[col, (-j) % 4], sent, l_recv, peer(col, j))
            remote(pbuf.at[0, col, 0], pbuf.at[0, col, (-j) % 4], sent, s2_recv.at[0, col], peer(col, j))
    for k in SINGLE:
        slot = (-k) % NZ
        remote(pbuf.at[0, :, 0], pbuf.at[slot, :, 0], sent, z_recv.at[ALONE[slot] - 1], at(dz=k))
    for src, dst, n in weights:
        remote(src, dst.at[c], sent, w_recv.at[n], partner)

    seen = set()

    def once(key):
        if key in seen:
            return False
        seen.add(key)
        return True

    def mb(k, col):
        lanes = iota((8, 128), 1) // BLK
        base = jnp.where(iota((8, 128), 0) < 4, lanes * CAP, 0).astype(F32)
        drain(lsend.at[:, pl.ds(1, 3)], l_recv)
        for col in range(2):
            for hi in range(2):
                t = [lmeta[col, s, hi].astype(F32) for s in range(4)]
                for lo in range(4):
                    turned = [t[s] if s == lo else pltpu.roll(t[s], BLK * ((s - lo) % 4), 1) for s in range(4)]
                    m = jnp.where(
                        lanes < 2, jnp.where(lanes == 0, turned[0], turned[1]), jnp.where(lanes == 2, turned[2], turned[3])
                    )
                    msrc[hi * 4 + lo, col] = (m + base).astype(BF)
        for k in DISTANT:
            slot = (-k) % NZ
            remote(msrc.at[k], mtab.at[slot], sent, m_recv.at[FAR[slot]], at(dz=k))

    def s2(k, col):
        if once(("z", k)):
            drain(pbuf.at[k, :, 0], z_recv.at[ALONE[k] - 1])
        for j in (2, 1, 3):
            remote(pbuf.at[k, col, 0], pbuf.at[k, col, (-j) % 4], sent, s2_recv.at[ALONE[k], col], peer(col, j))

    def table(k, col):
        if k == 0 or k in NEAR:
            return msrc[k, col].astype(F32)
        return mtab[k, col].astype(F32)

    def select(k, col, weighted):
        m = table(k, col)
        sixty = iota((64, 128), 0).astype(F32)
        parts = []
        for j in range(4):
            value = m[4 + j : 5 + j, :] if weighted else 1.0
            parts.append(jnp.where(sixty == m[j : j + 1, :], value, 0.0).astype(BF))
        return jnp.concatenate(parts, axis=0)

    def lined(k, col):
        if once(("s2", k, col)):
            if k in BUNDLE:
                drain(pbuf.at[k, col], b_recv.at[BUNDLE.index(k), col])
            else:
                drain(pbuf.at[k, col, pl.ds(1, 3)], s2_recv.at[ALONE[k], col])

    def zb(k, col):
        lined(0, col)
        for k in BUNDLE:
            slot = (-k) % NZ
            remote(pbuf.at[0, col], pbuf.at[slot, col], sent, b_recv.at[BUNDLE.index(slot), col], at(dz=k))

    def s3(k, col):
        source = 0 if k in NEAR else k
        lined(source, col)
        if k in DISTANT and once(("m", k)):
            drain(mtab.at[k], m_recv.at[FAR[k]])
        rows = pbuf[source, col].reshape(128, HALF)
        packed = jnp.dot(select(k, col, False), rows, preferred_element_type=F32).astype(BF)
        there = (-k) % NZ if k in NEAR else k
        i, core = PLACE[there], OWNER[there]

        def target(slot):
            return xbuf.at[i, c, 0, slot] if col == 0 else xbuf.at[i, c, 1, :, slot]

        pieces = [packed[64 * j : 64 * j + 64].reshape(4, CAP, HALF) for j in range(4)]
        for j in range(4):
            if j or k in NEAR:
                sbuf[k, col, j] = pieces[j]
        for j in (1, 3, 2, 0) if k in NEAR else (2, 1, 3):
            device = far(col, j, k if k in NEAR else 0, core)
            remote(sbuf.at[k, col, j], target((-j) % 4), sent, x_recv.at[i], device)
        if k not in NEAR:

            @pl.when(c == core)
            def _():
                if col == 0:
                    xbuf[i, c, 0, 0] = pieces[0]
                else:
                    xbuf[i, c, 1, :, 0] = pieces[0]

            @pl.when(c != core)
            def _():
                sbuf[k, col, 0] = pieces[0]
                remote(sbuf.at[k, col, 0], target(0), sent, x_recv.at[i], partner)

    def ga(i, h):
        if once(("x", i)):
            drain(wg.at[:, pl.ds(0, 256 if PAIRS[i][0] in NEAR else 224)], x_recv.at[i])
        if once("w"):
            drain(wg, w_sem.at[0])
            drain(wg, w_recv.at[0])
        rows = jnp.concatenate([xbuf[i, s, col].reshape(256, HALF) for s in range(2) for col in range(2)], axis=1)
        gate = jnp.minimum(jnp.dot(rows, wg[h], preferred_element_type=F32), 7.0)
        lin = jnp.clip(jnp.dot(rows, wu[h], preferred_element_type=F32), -7.0, 7.0)
        sig = 0.5 * jnp.tanh(0.851 * gate) + 0.5
        hid[i, h] = (gate * sig * (lin + 1.0)).astype(BF)

    def db(i, h):
        if once("d"):
            drain(wd.at[0], w_sem.at[1])
            drain(wd.at[0], w_recv.at[1])
        hidden = jnp.concatenate([hid[i, 0], hid[i, 1]], axis=1)
        done = jnp.dot(hidden, wd[h], preferred_element_type=F32).astype(BF)
        k0, k1 = PAIRS[i]
        close = k0 in NEAR
        k = k0 + c * (k1 - k0)
        there = lax.rem(NZ - k, NZ) if close else k
        for col in range(2):
            rows = done[:, col * HALF : (col + 1) * HALF].reshape(4, 4, CAP, HALF)
            pieces = [rows[j] if col == 0 else rows[:, j] for j in range(4)]
            for j in range(4):
                if j or close:
                    ysend[i, h, col, j] = pieces[j]
            for j in (1, 3, 2, 0) if close else (2, 1, 3):
                device = far(col, j, k if close else 0, h)
                remote(
                    ysend.at[i, h, col, j], r1buf.at[there, col, (-j) % 4], sent,
                    r1_recv.at[there, col], device,
                )
            if not close:

                @pl.when(c == h)
                def _():
                    r1buf[there, col, 0] = pieces[0]

                @pl.when(c != h)
                def _():
                    ysend[i, h, col, 0] = pieces[0]
                    remote(
                        ysend.at[i, h, col, 0], r1buf.at[there, col, 0], sent, r1_recv.at[there, col], partner
                    )

    def to_line(k, col, sums):
        pacc[k, col] = sums[:BLK]
        for j in range(1, 4):
            r2send[k, col, j - 1] = sums[BLK * j : BLK * j + BLK].astype(BF)
        for j in (2, 1, 3):
            remote(
                r2send.at[k, col, j - 1], r2buf.at[k, col, (-j) % 4 - 1], sent,
                r2_recv.at[LINED[k], col], peer(col, j),
            )

    def u7(k, col):
        if k in NEAR:
            drain(ysend.at[0, 0, 0], r1_recv.at[k, col])
        else:

            @pl.when(c == OWNER[k])
            def _():
                drain(ysend.at[0, 0, 0, pl.ds(1, 3)], r1_recv.at[k, col])

            @pl.when(c != OWNER[k])
            def _():
                drain(ysend.at[0, 0, 0], r1_recv.at[k, col])

        rows = r1buf[k, col].reshape(256, HALF)
        sums = lax.dot_general(select(k, col, True), rows, (((0,), (0,)), ((), ())), preferred_element_type=F32)
        if k == 0 or k in NEAR:
            if once(("e", col)):
                eacc[col] = sums
            else:
                eacc[col] += sums
        else:
            to_line(k, col, sums)

    def e2(k, col):
        to_line(0, col, eacc[col])

    def r8(k, col):
        drain(r2buf.at[k, col], r2_recv.at[LINED[k], col])
        total = pacc[k, col]
        for j in range(3):
            total = total + r2buf[k, col, j].astype(F32)
        slot = (-k) % NZ
        r3send[k, col] = total.astype(BF)
        remote(r3send.at[k, col], r3buf.at[slot, col], sent, r3_recv, at(dz=k))

    steps = (mb, s2, s3, ga, db, u7, r8, e2, zb)
    for step, k, col in SEQ:
        pl.when(c < 2)(lambda step=step, k=k, col=col: steps[step](k, col))

    part = []
    for col in range(2):
        drain(r2buf.at[0, col], r2_recv.at[0, col])
        total = pacc[0, col]
        for j in range(3):
            total = total + r2buf[0, col, j].astype(F32)
        part.append(total)
    drain(r3buf.at[pl.ds(0, NFAR)], r3_recv)
    for col in range(2):
        total = part[col]
        for k in DISTANT:
            total = total + r3buf[k, col].astype(F32)
        out_ref[:, col * HALF : (col + 1) * HALF] = total.astype(BF)

    drain(wg, sent)
    drain(wd.at[0], sent)
    drain(lsend.at[:, pl.ds(1, 3)], sent)
    drain(msrc.at[pl.ds(0, NFAR)], sent)
    drain(pbuf.at[pl.ds(0, len(SINGLE)), :, 0], sent)
    drain(pbuf.at[pl.ds(0, len(BUNDLE))], sent)
    drain(pbuf.at[pl.ds(0, len(SINGLE) + 1), :, pl.ds(1, 3)], sent)
    units = 56 + len(NEAR)
    for _ in range(2):
        drain(wg.at[:, pl.ds(0, 16 * units)], sent)
    drain(r2send.at[pl.ds(0, NFAR + 1)], sent)
    drain(r3send.at[pl.ds(0, NFAR)], sent)


def shards(tokens, norm_gain, routing, route_logits, w_gate, w_up, w_down):
    vmem = pltpu.VMEM
    dma = pltpu.SemaphoreType.DMA
    return pl.pallas_call(
        kernel,
        name="routed_layer",
        out_shape=vmem((BLK, 2 * HALF), BF),
        in_specs=[pl.BlockSpec(memory_space=pl.ANY)] * 7,
        out_specs=pl.BlockSpec(memory_space=vmem),
        scratch_shapes=[
            vmem((BLK, 1024), BF),
            vmem((1, 1024), F32),
            vmem((4, BLK), jnp.int32),
            vmem((4, BLK), F32),
            vmem((2, 1024, 512), BF),
            vmem((2, 1024, 512), BF),
            vmem((2, 1024, 512), BF),
            vmem((2, 4, 2, 8, 128), BF),
            vmem((2, 4, 2, 8, 128), BF),
            vmem((NZ, 2, 8, 128), BF),
            vmem((NZ, 2, 8, 128), BF),
            vmem((NZ, 2, 4, BLK, HALF), BF),
            vmem((NZ, 2, 4, 4, CAP, HALF), BF),
            vmem((4, 2, 2, 4, 4, CAP, HALF), BF),
            vmem((4, 2, 256, 512), BF),
            vmem((4, 2, 2, 4, 4, CAP, HALF), BF),
            vmem((NZ, 2, 4, 4, CAP, HALF), BF),
            vmem((2, 128, HALF), F32),
            vmem((NZ, 2, BLK, HALF), F32),
            vmem((NZ, 2, 3, BLK, HALF), BF),
            vmem((NZ, 2, 3, BLK, HALF), BF),
            vmem((NZ, 2, BLK, HALF), BF),
            vmem((NZ, 2, BLK, HALF), BF),
            dma((4,)),
            dma((2,)),
            dma((2,)),
            dma,
            dma,
            dma((NFAR,)),
            dma((len(SINGLE),)),
            dma((len(BUNDLE), 2)),
            dma((len(SINGLE) + 1, 2)),
            dma((4,)),
            dma((NZ, 2)),
            dma((NFAR + 1, 2)),
            dma,
        ],
        compiler_params=pltpu.CompilerParams(
            collective_id=0, has_side_effects=True, vmem_limit_bytes=60 * 1024 * 1024
        ),
    )(tokens, norm_gain.reshape(1, -1), routing.T, route_logits.T, w_gate[0], w_up[0], w_down[0])


def solution(mesh):
    return jax.shard_map(
        shards,
        mesh=mesh,
        in_specs=(
            P("ep", None),
            P(),
            P("ep", None),
            P("ep", None),
            P("ep", None, "tp"),
            P("ep", None, "tp"),
            P("ep", None, "tp"),
        ),
        out_specs=P("ep", "tp"),
        check_vma=False,
    )
```

```python
import jax
import jax.numpy as jnp
from jax import lax
from jax.experimental import pallas as pl
from jax.experimental.pallas import tpu as pltpu
from jax.sharding import PartitionSpec as P

MESH = pl.DeviceIdType.MESH
NX, NY, NZ = 4, 4, 8
CAP = 16
BLK = 32
HALF = 256
EPS = 1e-05
BF = jnp.bfloat16
F32 = jnp.float32
PAIRS = ((1, 0), (7, 2), (6, 3), (5, 4))
NEAR = ()
DISTANT = tuple(k for k in (1, 7, 2, 6, 3, 5, 4) if k not in NEAR)
NFAR = len(DISTANT)
BUNDLE = (3, 5)
SINGLE = tuple(k for k in DISTANT if k not in BUNDLE)
FAR = {k: n for n, k in enumerate(DISTANT)}
LINED = {k: n for n, k in enumerate((0,) + DISTANT)}
ALONE = {k: n for n, k in enumerate((0,) + SINGLE)}
OWNER = {k: c for pair in PAIRS for c, k in enumerate(pair)}
PLACE = {k: i for i, pair in enumerate(PAIRS) for k in pair}
SEQ = (
    (1, 7, 0), (1, 1, 0), (1, 1, 1), (0, 0, 0), (2, 0, 1), (8, 0, 1), (8, 0, 0), (2, 0, 0),
    (1, 2, 1), (1, 7, 1), (1, 6, 1), (1, 2, 0), (2, 1, 0), (2, 1, 1), (1, 4, 1), (1, 6, 0),
    (1, 4, 0), (2, 7, 1), (2, 2, 0), (2, 2, 1), (2, 7, 0), (2, 4, 1), (2, 6, 0), (3, 0, 0),
    (2, 5, 1), (2, 6, 1), (2, 4, 0), (2, 5, 0), (2, 3, 1), (2, 3, 0), (3, 1, 0), (3, 0, 1),
    (4, 0, 0), (3, 1, 1), (4, 1, 0), (3, 3, 0), (4, 1, 1), (3, 3, 1), (4, 3, 0), (3, 2, 0),
    (3, 2, 1), (4, 2, 0), (4, 3, 1), (4, 2, 1), (5, 4, 1), (5, 4, 0), (5, 5, 0), (5, 3, 1),
    (5, 3, 0), (5, 5, 1), (5, 6, 0), (5, 2, 1), (4, 0, 1), (6, 4, 0), (6, 4, 1), (5, 2, 0),
    (5, 6, 1), (5, 7, 1), (5, 1, 0), (6, 3, 1), (6, 5, 1), (5, 1, 1), (6, 3, 0), (5, 7, 0),
    (6, 6, 0), (6, 5, 0), (5, 0, 1), (7, 0, 1), (6, 2, 1), (6, 2, 0), (5, 0, 0), (7, 0, 0),
    (6, 6, 1), (6, 7, 1), (6, 1, 0), (6, 1, 1), (6, 7, 0),
)


def iota(shape, dim):
    return lax.broadcasted_iota(jnp.int32, shape, dim)


def kernel(
    tok_hbm, gain_hbm, ids_hbm, log_hbm, wg_hbm, wu_hbm, wd_hbm, out_ref,
    tok, gain, ids, logits, wg, wu, wd,
    lsend, lmeta, msrc, mtab, pbuf, sbuf, xbuf, hid, ysend, r1buf, eacc, pacc, r2send, r2buf, r3send, r3buf,
    in_sem, w_sem, w_recv, sent, l_recv, m_recv, z_recv, b_recv, s2_recv, x_recv, r1_recv, r2_recv, r3_recv,
):
    ep = lax.axis_index("ep")
    c = lax.axis_index("tp")
    x = lax.rem(ep, NX)
    y = lax.rem(ep // NX, NY)
    z = ep // (NX * NY)

    def at(dx=0, dy=0, dz=0, core=None):
        px = lax.rem(x + dx, NX)
        py = lax.rem(y + dy, NY)
        pz = lax.rem(z + dz, NZ)
        return ((pz * NY + py) * NX + px, c if core is None else core)

    partner = (ep, 1 - c)

    def peer(col, j):
        return at(dy=j) if col == 0 else at(dx=j)

    def far(col, j, dz, core):
        return at(dx=j, dz=dz, core=core) if col == 0 else at(dy=j, dz=dz, core=core)

    def remote(src, dst, send, recv, device):
        pltpu.make_async_remote_copy(
            src_ref=src, dst_ref=dst, send_sem=send, recv_sem=recv, device_id=device, device_id_type=MESH
        ).start()

    def drain(ref, sem):
        pltpu.make_async_copy(ref, ref, sem).wait()

    small = [
        pltpu.make_async_copy(tok_hbm, tok, in_sem.at[0]),
        pltpu.make_async_copy(gain_hbm, gain, in_sem.at[1]),
        pltpu.make_async_copy(ids_hbm, ids, in_sem.at[2]),
        pltpu.make_async_copy(log_hbm, logits, in_sem.at[3]),
    ]
    for copy in small:
        copy.start()

    barrier = pltpu.get_barrier_semaphore()
    both = (0, 1)
    friends = [partner]
    friends += [at(dy=j, core=o) for j in range(1, NY) for o in both]
    friends += [at(dx=j, core=o) for j in range(1, NX) for o in both]
    for k in NEAR:
        friends += [at(dz=k, core=o) for o in both]
        friends += [at(dy=j, dz=k, core=o) for j in range(1, NY) for o in both]
        friends += [at(dx=j, dz=k, core=o) for j in range(1, NX) for o in both]
    friends += [at(dz=k) for k in DISTANT]
    for friend in friends:
        pl.semaphore_signal(barrier, inc=1, device_id=friend, device_id_type=MESH)

    for copy in small:
        copy.wait()
    weights = ((wg_hbm, wg, 0), (wu_hbm, wu, 0), (wd_hbm, wd, 1))
    for src, dst, n in weights:
        pltpu.make_async_copy(src, dst.at[c], w_sem.at[n]).start()

    full = tok[...].astype(F32)
    scale = lax.rsqrt(jnp.mean(full * full, axis=-1, keepdims=True) + EPS)
    mine = pl.ds(pl.multiple_of(c * 512, 512), 512)
    normed = (tok[:, mine].astype(F32) * scale * gain[:, mine]).astype(BF)
    for col in range(2):
        pbuf[0, col, 0] = normed[:, col * HALF : (col + 1) * HALF]

    spread = (lax.rem(iota((BLK, 128), 1), BLK) == iota((BLK, 128), 0)).astype(BF)
    raw = logits[...]
    shifted = jnp.exp(raw - jnp.max(raw, axis=0, keepdims=True))
    probs = shifted / jnp.sum(shifted, axis=0, keepdims=True)
    ids_l = jnp.dot(ids[...].astype(F32).astype(BF), spread, preferred_element_type=F32)
    probs_l = jnp.dot(probs.astype(BF), spread, preferred_element_type=F32)
    row = iota((128, 128), 0)
    lane = iota((128, 128), 1)
    plane = lax.rem(z + lax.rem(row // 8, 2) * 4 + lane // BLK, NZ)
    group = lax.rem(row // 16, 4)
    near = lax.rem(row, 4)
    route_b = row < 64
    ex = lax.rem(x + jnp.where(route_b, near, group), NX)
    ey = lax.rem(y + jnp.where(route_b, group, near), NY)
    expert = (plane * 16 + ey * NX + ex).astype(F32)
    named = jnp.zeros((128, 128), F32)
    weight = jnp.zeros((128, 128), F32)
    for q in range(4):
        hit = expert == ids_l[q : q + 1, :]
        named = jnp.where(hit, 1.0, named)
        weight = jnp.where(hit, probs_l[q : q + 1, :], weight)
    before = ((row // BLK == lane // BLK) & (row < lane)).astype(BF)
    place = jnp.dot(named.astype(BF), before, preferred_element_type=F32)
    place = jnp.where(named > 0, place, -128.0)
    meta = jnp.where(lax.rem(row, 8) < 4, place, weight).astype(BF)
    for col in range(2):
        for g in range(4):
            for hi in range(2):
                start = col * 64 + g * 16 + hi * 8
                tile = meta[start : start + 8, :]
                if g:
                    lsend[col, g, hi] = tile
                else:
                    lmeta[col, 0, hi] = tile

    pl.semaphore_wait(barrier, len(friends))

    for col in range(2):
        for j in (2, 1, 3):
            remote(lsend.at[col, j], lmeta.at[col, (-j) % 4], sent, l_recv, peer(col, j))
            remote(pbuf.at[0, col, 0], pbuf.at[0, col, (-j) % 4], sent, s2_recv.at[0, col], peer(col, j))
    for k in SINGLE:
        slot = (-k) % NZ
        remote(pbuf.at[0, :, 0], pbuf.at[slot, :, 0], sent, z_recv.at[ALONE[slot] - 1], at(dz=k))
    for src, dst, n in weights:
        remote(src, dst.at[c], sent, w_recv.at[n], partner)

    seen = set()

    def once(key):
        if key in seen:
            return False
        seen.add(key)
        return True

    def mb(k, col):
        lanes = iota((8, 128), 1) // BLK
        base = jnp.where(iota((8, 128), 0) < 4, lanes * CAP, 0).astype(F32)
        drain(lsend.at[:, pl.ds(1, 3)], l_recv)
        for col in range(2):
            for hi in range(2):
                t = [lmeta[col, s, hi].astype(F32) for s in range(4)]
                for lo in range(4):
                    turned = [t[s] if s == lo else pltpu.roll(t[s], BLK * ((s - lo) % 4), 1) for s in range(4)]
                    m = jnp.where(
                        lanes < 2, jnp.where(lanes == 0, turned[0], turned[1]), jnp.where(lanes == 2, turned[2], turned[3])
                    )
                    msrc[hi * 4 + lo, col] = (m + base).astype(BF)
        for k in DISTANT:
            slot = (-k) % NZ
            remote(msrc.at[k], mtab.at[slot], sent, m_recv.at[FAR[slot]], at(dz=k))

    def s2(k, col):
        if once(("z", k)):
            drain(pbuf.at[k, :, 0], z_recv.at[ALONE[k] - 1])
        for j in (2, 1, 3):
            remote(pbuf.at[k, col, 0], pbuf.at[k, col, (-j) % 4], sent, s2_recv.at[ALONE[k], col], peer(col, j))

    def table(k, col):
        if k == 0 or k in NEAR:
            return msrc[k, col].astype(F32)
        return mtab[k, col].astype(F32)

    def select(k, col, weighted):
        m = table(k, col)
        sixty = iota((64, 128), 0).astype(F32)
        parts = []
        for j in range(4):
            value = m[4 + j : 5 + j, :] if weighted else 1.0
            parts.append(jnp.where(sixty == m[j : j + 1, :], value, 0.0).astype(BF))
        return jnp.concatenate(parts, axis=0)

    def lined(k, col):
        if once(("s2", k, col)):
            if k in BUNDLE:
                drain(pbuf.at[k, col], b_recv.at[BUNDLE.index(k), col])
            else:
                drain(pbuf.at[k, col, pl.ds(1, 3)], s2_recv.at[ALONE[k], col])

    def zb(k, col):
        lined(0, col)
        for k in BUNDLE:
            slot = (-k) % NZ
            remote(pbuf.at[0, col], pbuf.at[slot, col], sent, b_recv.at[BUNDLE.index(slot), col], at(dz=k))

    def s3(k, col):
        source = 0 if k in NEAR else k
        lined(source, col)
        if k in DISTANT and once(("m", k)):
            drain(mtab.at[k], m_recv.at[FAR[k]])
        rows = pbuf[source, col].reshape(128, HALF)
        packed = jnp.dot(select(k, col, False), rows, preferred_element_type=F32).astype(BF)
        there = (-k) % NZ if k in NEAR else k
        i, core = PLACE[there], OWNER[there]

        def target(slot):
            return xbuf.at[i, c, 0, slot] if col == 0 else xbuf.at[i, c, 1, :, slot]

        pieces = [packed[64 * j : 64 * j + 64].reshape(4, CAP, HALF) for j in range(4)]
        for j in range(4):
            if j or k in NEAR:
                sbuf[k, col, j] = pieces[j]
        for j in (1, 3, 2, 0) if k in NEAR else (2, 1, 3):
            device = far(col, j, k if k in NEAR else 0, core)
            remote(sbuf.at[k, col, j], target((-j) % 4), sent, x_recv.at[i], device)
        if k not in NEAR:

            @pl.when(c == core)
            def _():
                if col == 0:
                    xbuf[i, c, 0, 0] = pieces[0]
                else:
                    xbuf[i, c, 1, :, 0] = pieces[0]

            @pl.when(c != core)
            def _():
                sbuf[k, col, 0] = pieces[0]
                remote(sbuf.at[k, col, 0], target(0), sent, x_recv.at[i], partner)

    def ga(i, h):
        if once(("x", i)):
            drain(wg.at[:, pl.ds(0, 256 if PAIRS[i][0] in NEAR else 224)], x_recv.at[i])
        if once("w"):
            drain(wg, w_sem.at[0])
            drain(wg, w_recv.at[0])
        rows = jnp.concatenate([xbuf[i, s, col].reshape(256, HALF) for s in range(2) for col in range(2)], axis=1)
        gate = jnp.minimum(jnp.dot(rows, wg[h], preferred_element_type=F32), 7.0)
        lin = jnp.clip(jnp.dot(rows, wu[h], preferred_element_type=F32), -7.0, 7.0)
        sig = 0.5 * jnp.tanh(0.851 * gate) + 0.5
        hid[i, h] = (gate * sig * (lin + 1.0)).astype(BF)

    def db(i, h):
        if once("d"):
            drain(wd.at[0], w_sem.at[1])
            drain(wd.at[0], w_recv.at[1])
        hidden = jnp.concatenate([hid[i, 0], hid[i, 1]], axis=1)
        done = jnp.dot(hidden, wd[h], preferred_element_type=F32).astype(BF)
        k0, k1 = PAIRS[i]
        close = k0 in NEAR
        k = k0 + c * (k1 - k0)
        there = lax.rem(NZ - k, NZ) if close else k
        for col in range(2):
            rows = done[:, col * HALF : (col + 1) * HALF].reshape(4, 4, CAP, HALF)
            pieces = [rows[j] if col == 0 else rows[:, j] for j in range(4)]
            for j in range(4):
                if j or close:
                    ysend[i, h, col, j] = pieces[j]
            for j in (1, 3, 2, 0) if close else (2, 1, 3):
                device = far(col, j, k if close else 0, h)
                remote(
                    ysend.at[i, h, col, j], r1buf.at[there, col, (-j) % 4], sent,
                    r1_recv.at[there, col], device,
                )
            if not close:

                @pl.when(c == h)
                def _():
                    r1buf[there, col, 0] = pieces[0]

                @pl.when(c != h)
                def _():
                    ysend[i, h, col, 0] = pieces[0]
                    remote(
                        ysend.at[i, h, col, 0], r1buf.at[there, col, 0], sent, r1_recv.at[there, col], partner
                    )

    def to_line(k, col, sums):
        pacc[k, col] = sums[:BLK]
        for j in range(1, 4):
            r2send[k, col, j - 1] = sums[BLK * j : BLK * j + BLK].astype(BF)
        for j in (2, 1, 3):
            remote(
                r2send.at[k, col, j - 1], r2buf.at[k, col, (-j) % 4 - 1], sent,
                r2_recv.at[LINED[k], col], peer(col, j),
            )

    def u7(k, col):
        if k in NEAR:
            drain(ysend.at[0, 0, 0], r1_recv.at[k, col])
        else:

            @pl.when(c == OWNER[k])
            def _():
                drain(ysend.at[0, 0, 0, pl.ds(1, 3)], r1_recv.at[k, col])

            @pl.when(c != OWNER[k])
            def _():
                drain(ysend.at[0, 0, 0], r1_recv.at[k, col])

        rows = r1buf[k, col].reshape(256, HALF)
        sums = lax.dot_general(select(k, col, True), rows, (((0,), (0,)), ((), ())), preferred_element_type=F32)
        if k == 0 or k in NEAR:
            if once(("e", col)):
                eacc[col] = sums
            else:
                eacc[col] += sums
        else:
            to_line(k, col, sums)

    def e2(k, col):
        to_line(0, col, eacc[col])

    def r8(k, col):
        drain(r2buf.at[k, col], r2_recv.at[LINED[k], col])
        total = pacc[k, col]
        for j in range(3):
            total = total + r2buf[k, col, j].astype(F32)
        slot = (-k) % NZ
        r3send[k, col] = total.astype(BF)
        remote(r3send.at[k, col], r3buf.at[slot, col], sent, r3_recv, at(dz=k))

    steps = (mb, s2, s3, ga, db, u7, r8, e2, zb)
    for step, k, col in SEQ:
        pl.when(c < 2)(lambda step=step, k=k, col=col: steps[step](k, col))

    part = []
    for col in range(2):
        drain(r2buf.at[0, col], r2_recv.at[0, col])
        total = pacc[0, col]
        for j in range(3):
            total = total + r2buf[0, col, j].astype(F32)
        part.append(total)
    drain(r3buf.at[pl.ds(0, NFAR)], r3_recv)
    for col in range(2):
        total = part[col]
        for k in DISTANT:
            total = total + r3buf[k, col].astype(F32)
        out_ref[:, col * HALF : (col + 1) * HALF] = total.astype(BF)

    drain(wg, sent)
    drain(wd.at[0], sent)
    drain(lsend.at[:, pl.ds(1, 3)], sent)
    drain(msrc.at[pl.ds(0, NFAR)], sent)
    drain(pbuf.at[pl.ds(0, len(SINGLE)), :, 0], sent)
    drain(pbuf.at[pl.ds(0, len(BUNDLE))], sent)
    drain(pbuf.at[pl.ds(0, len(SINGLE) + 1), :, pl.ds(1, 3)], sent)
    units = 56 + len(NEAR)
    for _ in range(2):
        drain(wg.at[:, pl.ds(0, 16 * units)], sent)
    drain(r2send.at[pl.ds(0, NFAR + 1)], sent)
    drain(r3send.at[pl.ds(0, NFAR)], sent)


def shards(tokens, norm_gain, routing, route_logits, w_gate, w_up, w_down):
    vmem = pltpu.VMEM
    dma = pltpu.SemaphoreType.DMA
    return pl.pallas_call(
        kernel,
        name="routed_layer",
        out_shape=vmem((BLK, 2 * HALF), BF),
        in_specs=[pl.BlockSpec(memory_space=pl.ANY)] * 7,
        out_specs=pl.BlockSpec(memory_space=vmem),
        scratch_shapes=[
            vmem((BLK, 1024), BF),
            vmem((1, 1024), F32),
            vmem((4, BLK), jnp.int32),
            vmem((4, BLK), F32),
            vmem((2, 1024, 512), BF),
            vmem((2, 1024, 512), BF),
            vmem((2, 1024, 512), BF),
            vmem((2, 4, 2, 8, 128), BF),
            vmem((2, 4, 2, 8, 128), BF),
            vmem((NZ, 2, 8, 128), BF),
            vmem((NZ, 2, 8, 128), BF),
            vmem((NZ, 2, 4, BLK, HALF), BF),
            vmem((NZ, 2, 4, 4, CAP, HALF), BF),
            vmem((4, 2, 2, 4, 4, CAP, HALF), BF),
            vmem((4, 2, 256, 512), BF),
            vmem((4, 2, 2, 4, 4, CAP, HALF), BF),
            vmem((NZ, 2, 4, 4, CAP, HALF), BF),
            vmem((2, 128, HALF), F32),
            vmem((NZ, 2, BLK, HALF), F32),
            vmem((NZ, 2, 3, BLK, HALF), BF),
            vmem((NZ, 2, 3, BLK, HALF), BF),
            vmem((NZ, 2, BLK, HALF), BF),
            vmem((NZ, 2, BLK, HALF), BF),
            dma((4,)),
            dma((2,)),
            dma((2,)),
            dma,
            dma,
            dma((NFAR,)),
            dma((len(SINGLE),)),
            dma((len(BUNDLE), 2)),
            dma((len(SINGLE) + 1, 2)),
            dma((4,)),
            dma((NZ, 2)),
            dma((NFAR + 1, 2)),
            dma,
        ],
        compiler_params=pltpu.CompilerParams(
            collective_id=0, has_side_effects=True, vmem_limit_bytes=60 * 1024 * 1024
        ),
    )(tokens, norm_gain.reshape(1, -1), routing.T, route_logits.T, w_gate[0], w_up[0], w_down[0])


def solution(mesh):
    return jax.shard_map(
        shards,
        mesh=mesh,
        in_specs=(
            P("ep", None),
            P(),
            P("ep", None),
            P("ep", None),
            P("ep", None, "tp"),
            P("ep", None, "tp"),
            P("ep", None, "tp"),
        ),
        out_specs=P("ep", "tp"),
        check_vma=False,
    )
```

```python
import jax
import jax.numpy as jnp
from jax import lax
from jax.experimental import pallas as pl
from jax.experimental.pallas import tpu as pltpu
from jax.sharding import PartitionSpec as P

MESH = pl.DeviceIdType.MESH
NX, NY, NZ = 4, 4, 8
CAP = 16
BLK = 32
HALF = 256
EPS = 1e-05
BF = jnp.bfloat16
F32 = jnp.float32
PAIRS = ((1, 0), (7, 2), (6, 3), (5, 4))
NEAR = ()
DISTANT = tuple(k for k in (1, 7, 2, 6, 3, 5, 4) if k not in NEAR)
NFAR = len(DISTANT)
BUNDLE = (3, 5)
SINGLE = tuple(k for k in DISTANT if k not in BUNDLE)
FAR = {k: n for n, k in enumerate(DISTANT)}
LINED = {k: n for n, k in enumerate((0,) + DISTANT)}
ALONE = {k: n for n, k in enumerate((0,) + SINGLE)}
OWNER = {k: c for pair in PAIRS for c, k in enumerate(pair)}
PLACE = {k: i for i, pair in enumerate(PAIRS) for k in pair}
SEQ = (
    (1, 7, 1), (1, 1, 0), (0, 0, 0), (1, 1, 1), (1, 7, 0), (8, 0, 1), (8, 0, 0), (2, 0, 1),
    (2, 0, 0), (1, 2, 0), (1, 2, 1), (1, 6, 0), (1, 6, 1), (2, 1, 0), (2, 1, 1), (1, 4, 1),
    (1, 4, 0), (2, 2, 1), (2, 7, 0), (2, 7, 1), (2, 2, 0), (2, 4, 0), (2, 5, 1), (2, 6, 0),
    (2, 6, 1), (2, 4, 1), (2, 3, 1), (3, 0, 0), (2, 5, 0), (3, 0, 1), (2, 3, 0), (3, 1, 0),
    (4, 0, 0), (3, 1, 1), (4, 1, 0), (4, 1, 1), (3, 3, 0), (3, 3, 1), (4, 3, 0), (3, 2, 0),
    (3, 2, 1), (4, 2, 0), (4, 3, 1), (4, 2, 1), (5, 4, 0), (5, 4, 1), (5, 5, 1), (5, 2, 1),
    (5, 3, 0), (5, 5, 0), (5, 6, 0), (5, 3, 1), (4, 0, 1), (6, 4, 1), (5, 2, 0), (5, 6, 1),
    (5, 7, 1), (6, 5, 1), (6, 3, 0), (6, 4, 0), (6, 2, 1), (5, 1, 0), (6, 5, 0), (5, 1, 1),
    (5, 7, 0), (6, 3, 1), (6, 2, 0), (6, 6, 0), (5, 0, 0), (7, 0, 0), (5, 0, 1), (7, 0, 1),
    (6, 6, 1), (6, 7, 1), (6, 1, 0), (6, 1, 1), (6, 7, 0),
)


def iota(shape, dim):
    return lax.broadcasted_iota(jnp.int32, shape, dim)


def kernel(
    tok_hbm, gain_hbm, ids_hbm, log_hbm, wg_hbm, wu_hbm, wd_hbm, out_ref,
    tok, gain, ids, logits, wg, wu, wd,
    lsend, lmeta, msrc, mtab, pbuf, sbuf, xbuf, hid, ysend, r1buf, eacc, pacc, r2send, r2buf, r3send, r3buf,
    in_sem, w_sem, w_recv, sent, l_recv, m_recv, z_recv, b_recv, s2_recv, x_recv, r1_recv, r2_recv, r3_recv,
):
    ep = lax.axis_index("ep")
    c = lax.axis_index("tp")
    x = lax.rem(ep, NX)
    y = lax.rem(ep // NX, NY)
    z = ep // (NX * NY)

    def at(dx=0, dy=0, dz=0, core=None):
        px = lax.rem(x + dx, NX)
        py = lax.rem(y + dy, NY)
        pz = lax.rem(z + dz, NZ)
        return ((pz * NY + py) * NX + px, c if core is None else core)

    partner = (ep, 1 - c)

    def peer(col, j):
        return at(dy=j) if col == 0 else at(dx=j)

    def far(col, j, dz, core):
        return at(dx=j, dz=dz, core=core) if col == 0 else at(dy=j, dz=dz, core=core)

    def remote(src, dst, send, recv, device):
        pltpu.make_async_remote_copy(
            src_ref=src, dst_ref=dst, send_sem=send, recv_sem=recv, device_id=device, device_id_type=MESH
        ).start()

    def drain(ref, sem):
        pltpu.make_async_copy(ref, ref, sem).wait()

    small = [
        pltpu.make_async_copy(tok_hbm, tok, in_sem.at[0]),
        pltpu.make_async_copy(gain_hbm, gain, in_sem.at[1]),
        pltpu.make_async_copy(ids_hbm, ids, in_sem.at[2]),
        pltpu.make_async_copy(log_hbm, logits, in_sem.at[3]),
    ]
    for copy in small:
        copy.start()

    barrier = pltpu.get_barrier_semaphore()
    both = (0, 1)
    friends = [partner]
    friends += [at(dy=j, core=o) for j in range(1, NY) for o in both]
    friends += [at(dx=j, core=o) for j in range(1, NX) for o in both]
    for k in NEAR:
        friends += [at(dz=k, core=o) for o in both]
        friends += [at(dy=j, dz=k, core=o) for j in range(1, NY) for o in both]
        friends += [at(dx=j, dz=k, core=o) for j in range(1, NX) for o in both]
    friends += [at(dz=k) for k in DISTANT]
    for friend in friends:
        pl.semaphore_signal(barrier, inc=1, device_id=friend, device_id_type=MESH)

    for copy in small:
        copy.wait()
    weights = ((wg_hbm, wg, 0), (wu_hbm, wu, 0), (wd_hbm, wd, 1))
    for src, dst, n in weights:
        pltpu.make_async_copy(src, dst.at[c], w_sem.at[n]).start()

    full = tok[...].astype(F32)
    scale = lax.rsqrt(jnp.mean(full * full, axis=-1, keepdims=True) + EPS)
    mine = pl.ds(pl.multiple_of(c * 512, 512), 512)
    normed = (tok[:, mine].astype(F32) * scale * gain[:, mine]).astype(BF)
    for col in range(2):
        pbuf[0, col, 0] = normed[:, col * HALF : (col + 1) * HALF]

    spread = (lax.rem(iota((BLK, 128), 1), BLK) == iota((BLK, 128), 0)).astype(BF)
    raw = logits[...]
    shifted = jnp.exp(raw - jnp.max(raw, axis=0, keepdims=True))
    probs = shifted / jnp.sum(shifted, axis=0, keepdims=True)
    ids_l = jnp.dot(ids[...].astype(F32).astype(BF), spread, preferred_element_type=F32)
    probs_l = jnp.dot(probs.astype(BF), spread, preferred_element_type=F32)
    row = iota((128, 128), 0)
    lane = iota((128, 128), 1)
    plane = lax.rem(z + lax.rem(row // 8, 2) * 4 + lane // BLK, NZ)
    group = lax.rem(row // 16, 4)
    near = lax.rem(row, 4)
    route_b = row < 64
    ex = lax.rem(x + jnp.where(route_b, near, group), NX)
    ey = lax.rem(y + jnp.where(route_b, group, near), NY)
    expert = (plane * 16 + ey * NX + ex).astype(F32)
    named = jnp.zeros((128, 128), F32)
    weight = jnp.zeros((128, 128), F32)
    for q in range(4):
        hit = expert == ids_l[q : q + 1, :]
        named = jnp.where(hit, 1.0, named)
        weight = jnp.where(hit, probs_l[q : q + 1, :], weight)
    before = ((row // BLK == lane // BLK) & (row < lane)).astype(BF)
    place = jnp.dot(named.astype(BF), before, preferred_element_type=F32)
    place = jnp.where(named > 0, place, -128.0)
    meta = jnp.where(lax.rem(row, 8) < 4, place, weight).astype(BF)
    for col in range(2):
        for g in range(4):
            for hi in range(2):
                start = col * 64 + g * 16 + hi * 8
                tile = meta[start : start + 8, :]
                if g:
                    lsend[col, g, hi] = tile
                else:
                    lmeta[col, 0, hi] = tile

    pl.semaphore_wait(barrier, len(friends))

    for col in range(2):
        for j in (2, 1, 3):
            remote(pbuf.at[0, col, 0], pbuf.at[0, col, (-j) % 4], sent, s2_recv.at[0, col], peer(col, j))
            remote(lsend.at[col, j], lmeta.at[col, (-j) % 4], sent, l_recv, peer(col, j))
    for k in SINGLE:
        slot = (-k) % NZ
        remote(pbuf.at[0, :, 0], pbuf.at[slot, :, 0], sent, z_recv.at[ALONE[slot]], at(dz=k))
    for src, dst, n in weights:
        remote(src, dst.at[c], sent, w_recv.at[n], partner)

    seen = set()

    def once(key):
        if key in seen:
            return False
        seen.add(key)
        return True

    def mb(k, col):
        lanes = iota((8, 128), 1) // BLK
        base = jnp.where(iota((8, 128), 0) < 4, lanes * CAP, 0).astype(F32)
        drain(lsend.at[:, pl.ds(1, 3)], l_recv)
        for col in range(2):
            for hi in range(2):
                t = [lmeta[col, s, hi].astype(F32) for s in range(4)]
                for lo in range(4):
                    turned = [t[s] if s == lo else pltpu.roll(t[s], BLK * ((s - lo) % 4), 1) for s in range(4)]
                    m = jnp.where(
                        lanes < 2, jnp.where(lanes == 0, turned[0], turned[1]), jnp.where(lanes == 2, turned[2], turned[3])
                    )
                    msrc[hi * 4 + lo, col] = (m + base).astype(BF)
        for k in DISTANT:
            slot = (-k) % NZ
            remote(msrc.at[k], mtab.at[slot], sent, m_recv.at[FAR[slot]], at(dz=k))

    def s2(k, col):
        if once(("z", k)):
            drain(pbuf.at[k, :, 0], z_recv.at[ALONE[k]])
        for j in (2, 1, 3):
            remote(pbuf.at[k, col, 0], pbuf.at[k, col, (-j) % 4], sent, s2_recv.at[ALONE[k], col], peer(col, j))

    def table(k, col):
        if k == 0 or k in NEAR:
            return msrc[k, col].astype(F32)
        return mtab[k, col].astype(F32)

    def select(k, col, weighted):
        m = table(k, col)
        sixty = iota((64, 128), 0).astype(F32)
        parts = []
        for j in range(4):
            value = m[4 + j : 5 + j, :] if weighted else 1.0
            parts.append(jnp.where(sixty == m[j : j + 1, :], value, 0.0).astype(BF))
        return jnp.concatenate(parts, axis=0)

    def lined(k, col):
        if once(("s2", k, col)):
            if k in BUNDLE:
                drain(pbuf.at[k, col], b_recv.at[BUNDLE.index(k), col])
            else:
                drain(pbuf.at[k, col, pl.ds(1, 3)], s2_recv.at[ALONE[k], col])

    def zb(k, col):
        lined(0, col)
        for k in BUNDLE:
            slot = (-k) % NZ
            remote(pbuf.at[0, col], pbuf.at[slot, col], sent, b_recv.at[BUNDLE.index(slot), col], at(dz=k))

    def s3(k, col):
        source = 0 if k in NEAR else k
        lined(source, col)
        if k in DISTANT and once(("m", k)):
            drain(mtab.at[k], m_recv.at[FAR[k]])
        rows = pbuf[source, col].reshape(128, HALF)
        packed = jnp.dot(select(k, col, False), rows, preferred_element_type=F32).astype(BF)
        there = (-k) % NZ if k in NEAR else k
        i, core = PLACE[there], OWNER[there]

        def target(slot):
            return xbuf.at[i, c, 0, slot] if col == 0 else xbuf.at[i, c, 1, :, slot]

        pieces = [packed[64 * j : 64 * j + 64].reshape(4, CAP, HALF) for j in range(4)]
        for j in range(4):
            if j or k in NEAR:
                sbuf[k, col, j] = pieces[j]
        for j in (1, 3, 2, 0) if k in NEAR else (2, 1, 3):
            device = far(col, j, k if k in NEAR else 0, core)
            remote(sbuf.at[k, col, j], target((-j) % 4), sent, x_recv.at[i, c], device)
        if k not in NEAR:

            @pl.when(c == core)
            def _():
                if col == 0:
                    xbuf[i, c, 0, 0] = pieces[0]
                else:
                    xbuf[i, c, 1, :, 0] = pieces[0]

            @pl.when(c != core)
            def _():
                sbuf[k, col, 0] = pieces[0]
                remote(sbuf.at[k, col, 0], target(0), sent, x_recv.at[i, c], partner)

    def ga(i, h):
        if once(("x", i)):
            drain(sbuf.at[0] if PAIRS[i][0] in NEAR else sbuf.at[0, :, pl.ds(1, 3)], x_recv.at[i, c])
            drain(sbuf.at[0], x_recv.at[i, 1 - c])
        if once("w"):
            drain(wg, w_sem.at[0])
            drain(wg, w_recv.at[0])
        rows = jnp.concatenate([xbuf[i, s, col].reshape(256, HALF) for s in range(2) for col in range(2)], axis=1)
        gate = jnp.minimum(jnp.dot(rows, wg[h], preferred_element_type=F32), 7.0)
        lin = jnp.clip(jnp.dot(rows, wu[h], preferred_element_type=F32), -7.0, 7.0)
        sig = 0.5 * jnp.tanh(0.851 * gate) + 0.5
        hid[i, h] = (gate * sig * (lin + 1.0)).astype(BF)

    def db(i, h):
        if once("d"):
            drain(wd.at[0], w_sem.at[1])
            drain(wd.at[0], w_recv.at[1])
        hidden = jnp.concatenate([hid[i, 0], hid[i, 1]], axis=1)
        done = jnp.dot(hidden, wd[h], preferred_element_type=F32).astype(BF)
        k0, k1 = PAIRS[i]
        close = k0 in NEAR
        k = k0 + c * (k1 - k0)
        there = lax.rem(NZ - k, NZ) if close else k
        for col in range(2):
            rows = done[:, col * HALF : (col + 1) * HALF].reshape(4, 4, CAP, HALF)
            pieces = [rows[j] if col == 0 else rows[:, j] for j in range(4)]
            for j in range(4):
                if j or close:
                    ysend[i, h, col, j] = pieces[j]
            for j in (1, 3, 2, 0) if close else (2, 1, 3):
                device = far(col, j, k if close else 0, h)
                remote(
                    ysend.at[i, h, col, j], r1buf.at[there, col, (-j) % 4], sent,
                    r1_recv.at[there, col], device,
                )
            if not close:

                @pl.when(c == h)
                def _():
                    r1buf[there, col, 0] = pieces[0]

                @pl.when(c != h)
                def _():
                    ysend[i, h, col, 0] = pieces[0]
                    remote(
                        ysend.at[i, h, col, 0], r1buf.at[there, col, 0], sent, r1_recv.at[there, col], partner
                    )

    def to_line(k, col, sums):
        pacc[k, col] = sums[:BLK]
        for j in range(1, 4):
            r2send[k, col, j - 1] = sums[BLK * j : BLK * j + BLK].astype(BF)
        for j in (2, 1, 3):
            remote(
                r2send.at[k, col, j - 1], r2buf.at[k, col, (-j) % 4 - 1], sent,
                r2_recv.at[LINED[k], col], peer(col, j),
            )

    def u7(k, col):
        if k in NEAR:
            drain(ysend.at[0, 0, 0], r1_recv.at[k, col])
        else:

            @pl.when(c == OWNER[k])
            def _():
                drain(ysend.at[0, 0, 0, pl.ds(1, 3)], r1_recv.at[k, col])

            @pl.when(c != OWNER[k])
            def _():
                drain(ysend.at[0, 0, 0], r1_recv.at[k, col])

        rows = r1buf[k, col].reshape(256, HALF)
        sums = lax.dot_general(select(k, col, True), rows, (((0,), (0,)), ((), ())), preferred_element_type=F32)
        if k == 0 or k in NEAR:
            if once(("e", col)):
                eacc[col] = sums
            else:
                eacc[col] += sums
        else:
            to_line(k, col, sums)

    def e2(k, col):
        to_line(0, col, eacc[col])

    def r8(k, col):
        drain(r2buf.at[k, col], r2_recv.at[LINED[k], col])
        total = pacc[k, col]
        for j in range(3):
            total = total + r2buf[k, col, j].astype(F32)
        slot = (-k) % NZ
        r3send[k, col] = total.astype(BF)
        remote(r3send.at[k, col], r3buf.at[slot, col], sent, r3_recv, at(dz=k))

    steps = (mb, s2, s3, ga, db, u7, r8, e2, zb)
    for step, k, col in SEQ:
        pl.when(c < 2)(lambda step=step, k=k, col=col: steps[step](k, col))

    part = []
    for col in range(2):
        drain(r2buf.at[0, col], r2_recv.at[0, col])
        total = pacc[0, col]
        for j in range(3):
            total = total + r2buf[0, col, j].astype(F32)
        part.append(total)
    drain(r3buf.at[pl.ds(0, NFAR)], r3_recv)
    for col in range(2):
        total = part[col]
        for k in DISTANT:
            total = total + r3buf[k, col].astype(F32)
        out_ref[:, col * HALF : (col + 1) * HALF] = total.astype(BF)

    drain(wg, sent)
    drain(wd.at[0], sent)
    drain(lsend.at[:, pl.ds(1, 3)], sent)
    drain(msrc.at[pl.ds(0, NFAR)], sent)
    drain(pbuf.at[pl.ds(0, len(SINGLE)), :, 0], sent)
    drain(pbuf.at[pl.ds(0, len(BUNDLE))], sent)
    drain(pbuf.at[pl.ds(0, len(SINGLE) + 1), :, pl.ds(1, 3)], sent)
    units = 56 + len(NEAR)
    for _ in range(2):
        drain(wg.at[:, pl.ds(0, 16 * units)], sent)
    drain(r2send.at[pl.ds(0, NFAR + 1)], sent)
    drain(r3send.at[pl.ds(0, NFAR)], sent)


def shards(tokens, norm_gain, routing, route_logits, w_gate, w_up, w_down):
    vmem = pltpu.VMEM
    dma = pltpu.SemaphoreType.DMA
    return pl.pallas_call(
        kernel,
        name="routed_layer",
        out_shape=vmem((BLK, 2 * HALF), BF),
        in_specs=[pl.BlockSpec(memory_space=pl.ANY)] * 7,
        out_specs=pl.BlockSpec(memory_space=vmem),
        scratch_shapes=[
            vmem((BLK, 1024), BF),
            vmem((1, 1024), F32),
            vmem((4, BLK), jnp.int32),
            vmem((4, BLK), F32),
            vmem((2, 1024, 512), BF),
            vmem((2, 1024, 512), BF),
            vmem((2, 1024, 512), BF),
            vmem((2, 4, 2, 8, 128), BF),
            vmem((2, 4, 2, 8, 128), BF),
            vmem((NZ, 2, 8, 128), BF),
            vmem((NZ, 2, 8, 128), BF),
            vmem((NZ, 2, 4, BLK, HALF), BF),
            vmem((NZ, 2, 4, 4, CAP, HALF), BF),
            vmem((4, 2, 2, 4, 4, CAP, HALF), BF),
            vmem((4, 2, 256, 512), BF),
            vmem((4, 2, 2, 4, 4, CAP, HALF), BF),
            vmem((NZ, 2, 4, 4, CAP, HALF), BF),
            vmem((2, 128, HALF), F32),
            vmem((NZ, 2, BLK, HALF), F32),
            vmem((NZ, 2, 3, BLK, HALF), BF),
            vmem((NZ, 2, 3, BLK, HALF), BF),
            vmem((NZ, 2, BLK, HALF), BF),
            vmem((NZ, 2, BLK, HALF), BF),
            dma((4,)),
            dma((2,)),
            dma((2,)),
            dma,
            dma,
            dma((NFAR,)),
            dma((len(SINGLE) + 1,)),
            dma((len(BUNDLE), 2)),
            dma((len(SINGLE) + 1, 2)),
            dma((4, 2)),
            dma((NZ, 2)),
            dma((NFAR + 1, 2)),
            dma,
        ],
        compiler_params=pltpu.CompilerParams(
            collective_id=0, has_side_effects=True, vmem_limit_bytes=60 * 1024 * 1024
        ),
    )(tokens, norm_gain.reshape(1, -1), routing.T, route_logits.T, w_gate[0], w_up[0], w_down[0])


def solution(mesh):
    return jax.shard_map(
        shards,
        mesh=mesh,
        in_specs=(
            P("ep", None),
            P(),
            P("ep", None),
            P("ep", None),
            P("ep", None, "tp"),
            P("ep", None, "tp"),
            P("ep", None, "tp"),
        ),
        out_specs=P("ep", "tp"),
        check_vma=False,
    )
```
